32 devices in a mesh: sp: 16 (over z, y, x), tp: 2 (over core).
Axes of the slice: x: 2, y: 2, z: 4, core: 2. Of those that a mesh axis runs over, the one named last changes fastest.
Arguments:
- tokens: bfloat16 [4096, 2048], P(('sp', 'tp')), may hold values from -6 to 6
- norm_gain: float32 [2048], replicated, may hold values from 0.1 to 1.9
- w_query: bfloat16 [2048, 2048], P('sp', 'tp'), may hold values from -0.125 to 0.125
- w_key: bfloat16 [2048, 2048], P('sp', 'tp'), may hold values from -0.125 to 0.125
- w_value: bfloat16 [2048, 4096], P('sp', 'tp'), may hold values from -0.125 to 0.125
- w_rank_down: bfloat16 [2048, 16], replicated, may hold values from -0.125 to 0.125
- w_rank_up: bfloat16 [16, 2048], P(None, 'tp'), may hold values from -1.5 to 1.5
- gate_bias: float32 [2048], P('tp')
- decay_shift: float32 [4096], P('sp'), may hold values from -1 to 0
- out_gain: float32 [512], replicated, may hold values from 0.1 to 1.9
- w_out: bfloat16 [4096, 2048], P('tp', 'sp'), may hold values from -0.09375 to 0.09375
Outputs:
- mixed: bfloat16 [4096, 2048], P(('sp', 'tp'))
The draws below stay inside these ranges and needn't reach their ends.
All inputs are finite; a program needn't handle non-finite values.
Results may differ from the reference program's by a relative error of at most 0.015.
Values may be sent and summed in bfloat16 or wider, within the bound.
No kernel may reach another device: no remote copies, remote signals or barrier semaphores. Data moves between devices by JAX's collectives and lax.ppermute only.
A program may use at most 128 MiB of HBM per device.

```python
import jax
import jax.numpy as jnp
from jax import lax

D = 2048
HEADS = 8
DK = 256
DV = 512
RANK = 16
TAU = 16
BLOCK = 64
STRETCH = 256
TOKENS = 4096
KEYS = 2048
VALS = 4096
N_SP = 16
N_TP = 2


def draw_gate_bias(key, part):
    first, second, third = jax.random.split(key, 3)
    share = 0.5
    slow_head = jax.random.uniform(first, (HEADS,)) < share
    slow = jnp.log(2.0 * TOKENS / TAU) + jax.random.uniform(second, (HEADS, DK), minval=-0.5, maxval=0.5)
    fast = jax.random.uniform(third, (HEADS, DK), minval=0.5, maxval=1.5)
    return jnp.where(slow_head[:, None], slow, fast).reshape(HEADS * DK).astype(jnp.float32)


def draw_decay_shift(key, part):
    first, second, third, fourth = jax.random.split(key, 4)
    stretches = TOKENS // STRETCH
    level = jnp.exp(jax.random.uniform(first, (stretches,), minval=jnp.log(0.1), maxval=0.0))
    spread = jax.random.uniform(second, (TOKENS,), minval=0.5, maxval=1.5)
    per_position = -jnp.repeat(level, STRETCH) * spread / TOKENS
    spots = jax.random.randint(third, (3,), 0, TOKENS)
    drops = jnp.log(jax.random.uniform(fourth, (3,), minval=0.5, maxval=0.8))
    return per_position.at[spots].add(drops).astype(jnp.float32)


def shard_levels(stream_key, dims, cuts, least, top_value):
    def one(axis_at, parts):
        steps = jax.random.uniform(jax.random.fold_in(jax.random.fold_in(stream_key, 6), axis_at), (parts,), jnp.float32, least / len(cuts), top_value / len(cuts))
        return jnp.repeat(jnp.exp(steps), dims[axis_at] // parts).reshape((-1,) + (1,) * (len(dims) - axis_at - 1))

    factor_of = one(*cuts[0])
    for cut in cuts[1:]:
        factor_of = factor_of * one(*cut)
    return factor_of


def noise(own_key, extent, deviation, most, cuts=(), kind=jnp.bfloat16):
    array = deviation * jax.random.normal(own_key, extent, jnp.float32)
    if cuts:
        array = array * shard_levels(own_key, extent, cuts, -0.22, 0.18)
    return jnp.clip(array, -most, most).astype(kind)


def setup_inputs(seed: int = 0) -> dict:
    splits = jax.random.split(jax.random.key(seed), 12)
    tokens = noise(splits[0], (TOKENS, D), 1.0, 6.0, ((0, 32),))
    norm_gain = jnp.clip(1.0 + 0.18 * jax.random.normal(splits[1], (D,), jnp.float32), 0.1, 1.9)
    w_query = noise(splits[2], (D, KEYS), D ** -0.5, 0.125, ((0, 16), (1, 2)))
    w_key = noise(splits[3], (D, KEYS), D ** -0.5, 0.125, ((0, 16), (1, 2)))
    w_value = noise(splits[4], (D, VALS), D ** -0.5, 0.125, ((0, 16), (1, 2)))
    w_rank_down = noise(splits[5], (D, RANK), D ** -0.5, 0.125)
    w_rank_up = noise(splits[6], (RANK, KEYS), RANK ** -0.5, 1.5, ((1, 2),))
    gate_bias = draw_gate_bias(jax.random.fold_in(splits[11], 71), 0)
    decay_shift = draw_decay_shift(jax.random.fold_in(splits[11], 71), 0)
    out_gain = jnp.clip(1.0 + 0.18 * jax.random.normal(splits[9], (DV,), jnp.float32), 0.1, 1.9)
    w_out = noise(splits[10], (VALS, D), VALS ** -0.5, 0.09375, ((0, 2), (1, 16)))
    return dict(tokens=tokens, norm_gain=norm_gain, w_query=w_query, w_key=w_key, w_value=w_value, w_rank_down=w_rank_down, w_rank_up=w_rank_up, gate_bias=gate_bias, decay_shift=decay_shift, out_gain=out_gain, w_out=w_out)


EPS = 1e-06

def rms_rows(values, gain):
    wide = values.astype(jnp.float32)
    return wide * lax.rsqrt(lax.optimization_barrier(jnp.mean(wide * wide, axis=-1, keepdims=True)) + EPS) * gain

def narrow(values):
    return lax.optimization_barrier(values.astype(jnp.bfloat16)).astype(jnp.float32)

def local_pass(query, key, value, log_decay, state):
    rows, heads, width = query.shape
    blocks = rows // BLOCK

    def split(tensor):
        return tensor.reshape((blocks, BLOCK) + tensor.shape[1:])
    causal = jnp.tril(jnp.ones((BLOCK, BLOCK), dtype=bool))

    def step(carry, inputs):
        q_blk, k_blk, v_blk, g_blk = inputs
        cumul = jnp.cumsum(g_blk, axis=0)
        centre = cumul - cumul[BLOCK // 2]
        q_scaled = narrow(q_blk * jnp.exp(centre))
        k_scaled = narrow(k_blk * jnp.exp(-centre))
        scores = jnp.einsum('ihd,jhd->hij', q_scaled, k_scaled)
        scores = narrow(jnp.where(causal[None], scores, 0.0))
        within = jnp.einsum('hij,jhe->ihe', scores, v_blk)
        final = cumul[-1]
        decayed = narrow(k_blk * jnp.exp(final - cumul))
        nxt = jnp.exp(final)[:, :, None] * carry + jnp.einsum('jhd,jhe->hde', decayed, v_blk)
        return (nxt, (within, q_blk * jnp.exp(cumul), final, carry))
    carry, (within, reach, finals, starts) = lax.scan(step, state, (split(query), split(key), split(value), split(log_decay)))
    return (within, reach, finals, starts, carry)

def read_out(reach, starts):
    blocks, block, heads, width = reach.shape
    result = jnp.einsum('nihd,nhde->nihe', narrow(reach), narrow(starts))
    return result.reshape(blocks * block, heads, -1)

def reference(tokens, norm_gain, w_query, w_key, w_value, w_rank_down, w_rank_up, gate_bias, decay_shift, out_gain, w_out):
    group_width = HEADS // N_TP * DV

    def segment(state, inputs):
        rows, shift = inputs
        normed = rms_rows(rows, norm_gain).astype(jnp.bfloat16)
        query = jnp.dot(normed, w_query, preferred_element_type=jnp.float32).astype(jnp.bfloat16)
        keyed = jnp.dot(normed, w_key, preferred_element_type=jnp.float32).astype(jnp.bfloat16)
        valued = jnp.dot(normed, w_value, preferred_element_type=jnp.float32).astype(jnp.bfloat16)
        rank = jnp.dot(normed, w_rank_down, preferred_element_type=jnp.float32).astype(jnp.bfloat16)
        pre = jnp.dot(rank, w_rank_up, preferred_element_type=jnp.float32) + gate_bias
        log_decay = jax.nn.log_sigmoid(pre) / TAU + shift[:, None]
        q_heads = query.astype(jnp.float32).reshape(STRETCH, HEADS, DK) * DK ** (-0.5)
        k_heads = keyed.astype(jnp.float32).reshape(STRETCH, HEADS, DK)
        v_heads = valued.astype(jnp.float32).reshape(STRETCH, HEADS, DV)
        within, reach, _, starts, state = local_pass(q_heads, k_heads, v_heads, log_decay.reshape(STRETCH, HEADS, DK), state)
        attended = within.reshape(STRETCH, HEADS, DV) + read_out(reach, starts)
        shaped = rms_rows(attended, out_gain).astype(jnp.bfloat16).reshape(STRETCH, VALS)
        total = jnp.zeros((STRETCH, D), jnp.float32)
        for group in range(N_TP):
            lower = group * group_width
            part = jnp.dot(shaped[:, lower:lower + group_width], w_out[lower:lower + group_width], preferred_element_type=jnp.float32).astype(jnp.bfloat16)
            total = total + lax.optimization_barrier(part).astype(jnp.float32)
        return (state, total.astype(jnp.bfloat16))
    start = jnp.zeros((HEADS, DK, DV), jnp.float32)
    _, mixed = lax.scan(segment, start, (tokens.reshape(N_SP, STRETCH, D), decay_shift.reshape(N_SP, STRETCH)))
    return mixed.reshape(TOKENS, D)
```

```python
import jax
import jax.numpy as jnp
from jax import lax
from jax.sharding import PartitionSpec as P

DK = 256
DV = 512
TAU = 16
BLOCK = 64
EPS = 1e-06
SHORT = 8


def rms_rows(values, gain):
    wide = values.astype(jnp.float32)
    return wide * lax.rsqrt(jnp.mean(wide * wide, axis=-1, keepdims=True) + EPS) * gain


def partner(index, step, count):
    if count & (count - 1) == 0:
        return index ^ step
    return (step - index) % count


def plane_pairs(n_sp, n_p, step):
    return [(s, s // n_p * n_p + partner(s % n_p, step, n_p)) for s in range(n_sp)]


def gather_blocks(value, axis, index, count, pairs_of):
    out = jnp.zeros((count,) + value.shape, value.dtype)
    for step in range(count):
        got = value if pairs_of(step) is None else lax.ppermute(value, axis, pairs_of(step))
        out = lax.dynamic_update_index_in_dim(out, got, partner(index, step, count), 0)
    return out


def ring(value, n_sp, n_p):
    held = [value]
    for _ in range(n_sp // n_p - 1):
        held.append(lax.ppermute(held[-1], "sp", [(s, (s + n_p) % n_sp) for s in range(n_sp)]))
    return held


def gather_planes(value, n_sp, n_p):
    lines = [[i + j * n_p for j in range(n_sp // n_p)] for i in range(n_p)]
    return lax.all_gather(value, "sp", axis_index_groups=lines)


def attend(query, key, value, log_decay):
    rows, _ = query.shape
    blocks = rows // BLOCK

    def split(tensor):
        return tensor.reshape((blocks, BLOCK) + tensor.shape[1:])

    q, k, v, g = split(query), split(key), split(value), split(log_decay)
    causal = jnp.tril(jnp.ones((BLOCK, BLOCK), dtype=bool))
    cumul = jnp.cumsum(g, axis=1)
    centre = cumul - cumul[:, BLOCK // 2 : BLOCK // 2 + 1]
    q_scaled = (q * jnp.exp(centre)).astype(jnp.bfloat16)
    k_scaled = (k * jnp.exp(-centre)).astype(jnp.bfloat16)
    scores = jnp.einsum("nid,njd->nij", q_scaled, k_scaled, preferred_element_type=jnp.float32)
    scores = jnp.where(causal[None], scores, 0.0).astype(jnp.bfloat16)
    within = jnp.einsum("nij,nje->nie", scores, v, preferred_element_type=jnp.float32)
    final = cumul[:, -1]
    decayed = (k * jnp.exp(final[:, None] - cumul)).astype(jnp.bfloat16)
    added = jnp.einsum("njd,nje->nde", decayed, v, preferred_element_type=jnp.float32)
    state = jnp.zeros((DK, DV), jnp.float32)
    starts = []
    for n in range(blocks):
        starts.append(state.astype(jnp.bfloat16))
        state = jnp.exp(final[n])[:, None] * state + added[n]
    reach = (q * jnp.exp(cumul)).astype(jnp.bfloat16)
    before = jnp.cumsum(final, axis=0) - final
    far = (q * jnp.exp(cumul + before[:, None])).astype(jnp.bfloat16)
    within = within + jnp.einsum("nid,nde->nie", reach, jnp.stack(starts), preferred_element_type=jnp.float32)
    return within.reshape(rows, -1), far.reshape(rows, -1), state, jnp.sum(final, axis=0)


def entering(state, total, n_sp, n_p, z):
    n_z = n_sp // n_p
    if n_z > SHORT:
        step = 1
        while step < n_z:
            pairs = [(s, s + step * n_p) for s in range(n_sp - step * n_p)]
            state, total = (
                state + jnp.exp(total)[:, None] * lax.ppermute(state, "sp", pairs),
                total + lax.ppermute(total, "sp", pairs),
            )
            step *= 2
        return lax.ppermute(state, "sp", [(s, s + n_p) for s in range(n_sp - n_p)])
    sent = state.astype(jnp.bfloat16)
    result = jnp.zeros(state.shape, jnp.float32)
    since = jnp.zeros(total.shape, jnp.float32)
    for step in range(1, n_z):
        pairs = [(s, s + step * n_p) for s in range(n_sp - step * n_p)]
        far, decay = lax.ppermute(sent, "sp", pairs), lax.ppermute(total, "sp", pairs)
        result = result + jnp.exp(since)[:, None] * far.astype(jnp.float32)
        since = since + decay
    return result


def on_device(
    tokens,
    norm_gain,
    w_query,
    w_key,
    w_value,
    w_rank_down,
    w_rank_up,
    gate_bias,
    decay_shift,
    out_gain,
    w_out,
):
    n_sp, n_tp = lax.axis_size("sp"), lax.axis_size("tp")
    sp, tp = lax.axis_index("sp"), lax.axis_index("tp")
    n_p = w_query.shape[1] // DK
    n_z = n_sp // n_p
    p, z = sp % n_p, sp // n_p
    width = tokens.shape[1]
    groups = [[i * n_p + j for j in range(n_p)] for i in range(n_z)]

    def plane_of(step):
        return plane_pairs(n_sp, n_p, step) if step else None

    def core_of(step):
        return [(t, partner(t, step, n_tp)) for t in range(n_tp)] if step else None

    def exchange(value):
        if n_p == 1:
            return value
        return lax.all_to_all(value, "sp", 0, 0, axis_index_groups=groups, tiled=True)

    rows = w_query.shape[0]
    packed = jnp.concatenate(
        [
            w_query.reshape(rows, n_p, DK),
            w_key.reshape(rows, n_p, DK),
            w_value.reshape(rows, n_p, DV),
        ],
        axis=2,
    ).transpose(1, 0, 2)
    short = n_z <= SHORT
    weights = exchange(packed).reshape(n_p * rows, 2 * DK + DV)
    out_rows = w_out.shape[0] // n_p
    outs = exchange(w_out.reshape(n_p, out_rows, w_out.shape[1]))
    if short:
        depth = n_p * rows
        weights, outs = ring(weights, n_sp, n_p), ring(outs, n_sp, n_p)
    else:
        depth = n_sp * rows
        weights = [gather_planes(weights, n_sp, n_p).reshape(depth, 2 * DK + DV)]
        outs = [gather_planes(outs, n_sp, n_p).reshape(n_sp, out_rows, w_out.shape[1])]

    normed = rms_rows(tokens, norm_gain).astype(jnp.bfloat16)
    plane = gather_blocks(normed, "sp", p, n_p, plane_of)
    whole = gather_blocks(plane, "tp", tp, n_tp, core_of)
    span = n_p * n_tp * tokens.shape[0]
    whole = whole.transpose(1, 0, 2, 3).reshape(span, width)
    shift = gather_blocks(decay_shift, "sp", p, n_p, plane_of).reshape(span)

    joined = jnp.zeros((span, 2 * DK + DV), jnp.float32)
    for step, block in enumerate(weights):
        part = lax.dynamic_slice_in_dim(whole, (z - step) % n_z * depth if short else 0, depth, axis=1)
        joined = joined + jnp.dot(part, block, preferred_element_type=jnp.float32)
    joined = joined.astype(jnp.bfloat16)
    query = joined[:, :DK].astype(jnp.float32) * DK ** (-0.5)
    key = joined[:, DK : 2 * DK].astype(jnp.float32)
    value = joined[:, 2 * DK :]
    rank = jnp.dot(whole, w_rank_down, preferred_element_type=jnp.float32).astype(jnp.bfloat16)
    up = lax.dynamic_slice_in_dim(w_rank_up, p * DK, DK, axis=1)
    bias = lax.dynamic_slice_in_dim(gate_bias, p * DK, DK, axis=0)
    pre = jnp.dot(rank, up, preferred_element_type=jnp.float32) + bias
    log_decay = jax.nn.log_sigmoid(pre) / TAU + shift[:, None]

    near, far, state, total = attend(query, key, value, log_decay)
    carried = entering(state, total, n_sp, n_p, z).astype(jnp.bfloat16)
    attended = near + jnp.dot(far, carried, preferred_element_type=jnp.float32)
    shaped = rms_rows(attended, out_gain).astype(jnp.bfloat16)

    blocks = jnp.concatenate(
        [jnp.einsum("tk,pkc->tpc", shaped, part, preferred_element_type=jnp.float32) for part in outs], axis=1
    ).astype(jnp.bfloat16)
    blocks = blocks.reshape(n_p, n_tp, tokens.shape[0], width)
    mine = lax.dynamic_index_in_dim(blocks, tp, 1, keepdims=False).astype(jnp.float32)
    for step in range(1, n_tp):
        part = lax.dynamic_index_in_dim(blocks, partner(tp, step, n_tp), 1, keepdims=False)
        mine = mine + lax.ppermute(part, "tp", core_of(step)).astype(jnp.float32)
    mine = mine.astype(jnp.bfloat16)
    total_here = lax.dynamic_index_in_dim(mine, p, 0, keepdims=False).astype(jnp.float32)
    for step in range(1, n_p):
        part = lax.dynamic_index_in_dim(mine, partner(p, step, n_p), 0, keepdims=False)
        total_here = total_here + lax.ppermute(part, "sp", plane_of(step)).astype(jnp.float32)
    mixed = total_here.astype(jnp.bfloat16)
    if not short:
        return mixed
    mixed = mixed.reshape(tokens.shape[0], n_z, width // n_z)
    order = (z - jnp.arange(n_z)) % n_z
    return jnp.take(mixed, order, axis=1).reshape(tokens.shape[0], width)


def solution(mesh):
    return jax.shard_map(
        on_device,
        mesh=mesh,
        in_specs=(
            P(("sp", "tp"), None),
            P(),
            P("sp", "tp"),
            P("sp", "tp"),
            P("sp", "tp"),
            P(),
            P(None, "tp"),
            P("tp"),
            P("sp"),
            P(),
            P("tp", "sp"),
        ),
        out_specs=P(("sp", "tp"), None),
        check_vma=False,
    )
```

```python
import jax
import jax.numpy as jnp
from jax import lax
from jax.experimental import pallas as pl
from jax.experimental.pallas import tpu as pltpu
from jax.sharding import PartitionSpec as P


DK = 256
DV = 512
TAU = 16
BLOCK = 64
EPS = 1e-06
SHORT = 8
CUTS = 2


def rms_rows(values, gain):
    wide = values.astype(jnp.float32)
    return wide * lax.rsqrt(jnp.mean(wide * wide, axis=-1, keepdims=True) + EPS) * gain


def partner(index, step, count):
    if count & (count - 1) == 0:
        return index ^ step
    return (step - index) % count


def plane_pairs(n_sp, n_p, step):
    return [(s, s // n_p * n_p + partner(s % n_p, step, n_p)) for s in range(n_sp)]


def gather_blocks(value, axis, index, count, pairs_of):
    out = jnp.zeros((count,) + value.shape, value.dtype)
    for step in range(count):
        got = value if pairs_of(step) is None else lax.ppermute(value, axis, pairs_of(step))
        out = lax.dynamic_update_index_in_dim(out, got, partner(index, step, count), 0)
    return out


def gather_planes(value, n_sp, n_p):
    lines = [[i + j * n_p for j in range(n_sp // n_p)] for i in range(n_p)]
    return lax.all_gather(value, "sp", axis_index_groups=lines)


def pack_kernel(q_ref, k_ref, v_ref, out_ref):
    out_ref[0, :, :DK] = q_ref[...]
    out_ref[0, :, DK : 2 * DK] = k_ref[...]
    out_ref[0, :, 2 * DK :] = v_ref[...]


def pack(w_query, w_key, w_value):
    rows = w_query.shape[0]
    heads = w_query.shape[1] // DK
    return pl.pallas_call(
        pack_kernel,
        grid=(heads,),
        in_specs=[
            pl.BlockSpec((rows, DK), lambda h: (0, h)),
            pl.BlockSpec((rows, DK), lambda h: (0, h)),
            pl.BlockSpec((rows, DV), lambda h: (0, h)),
        ],
        out_specs=pl.BlockSpec((1, rows, 2 * DK + DV), lambda h: (h, 0, 0)),
        out_shape=jax.ShapeDtypeStruct((heads, rows, 2 * DK + DV), jnp.bfloat16),
        name="pack",
    )(w_query, w_key, w_value)


def mm(left, right, dims):
    return lax.dot_general(left, right, (dims, ((), ())), preferred_element_type=jnp.float32)


def attend_kernel(joined_ref, cumul_ref, before_ref, near_ref, far_ref, state_ref):
    blocks = joined_ref.shape[0] // BLOCK
    row = lax.broadcasted_iota(jnp.int32, (BLOCK, BLOCK), 0)
    column = lax.broadcasted_iota(jnp.int32, (BLOCK, BLOCK), 1)
    for n in range(blocks):
        span = slice(n * BLOCK, (n + 1) * BLOCK)
        q = joined_ref[span, :DK].astype(jnp.float32) * DK ** (-0.5)
        k = joined_ref[span, DK : 2 * DK].astype(jnp.float32)
        v = joined_ref[span, 2 * DK :]
        cumul = cumul_ref[span, :]
        centre = cumul - cumul[BLOCK // 2 : BLOCK // 2 + 1, :]
        final = cumul[BLOCK - 1 :, :]
        q_scaled = (q * jnp.exp(centre)).astype(jnp.bfloat16)
        k_scaled = (k * jnp.exp(-centre)).astype(jnp.bfloat16)
        scores = mm(q_scaled, k_scaled, ((1,), (1,)))
        scores = jnp.where(row >= column, scores, 0.0).astype(jnp.bfloat16)
        near = mm(scores, v, ((1,), (0,)))
        reach = q * jnp.exp(cumul)
        if n:
            near = near + mm(reach.astype(jnp.bfloat16), state_ref[...].astype(jnp.bfloat16), ((1,), (1,)))
        near_ref[span, :] = near
        far_ref[span, :] = (reach * jnp.exp(before_ref[n : n + 1, :])).astype(jnp.bfloat16)
        if n < blocks - 1:
            decayed = (k * jnp.exp(final - cumul)).astype(jnp.bfloat16)
            added = mm(v, decayed, ((0,), (0,)))
            state_ref[...] = state_ref[...] * jnp.exp(final) + added if n else added


def attend(joined, cumul, before):
    rows = joined.shape[0]
    return pl.pallas_call(
        attend_kernel,
        out_shape=(
            jax.ShapeDtypeStruct((rows, DV), jnp.float32),
            jax.ShapeDtypeStruct((rows, DK), jnp.bfloat16),
        ),
        scratch_shapes=[pltpu.VMEM((DV, DK), jnp.float32)],
        compiler_params=pltpu.CompilerParams(vmem_limit_bytes=40 << 20),
        cost_estimate=pl.CostEstimate(flops=5_000_000_000, transcendentals=2_000_000, bytes_accessed=6_000_000),
        name="attend",
    )(joined, cumul, before)


def finish_kernel(index_ref, near_ref, far_ref, carried_ref, gain_ref, out_ref):
    parts, rows = near_ref.shape[0], near_ref.shape[2]
    for i in range(parts):
        attended = near_ref[i, 0] + mm(far_ref[i, 0], carried_ref[...], ((1,), (0,)))
        scale = lax.rsqrt(jnp.mean(attended * attended, axis=-1, keepdims=True) + EPS)
        out_ref[0, i * rows : (i + 1) * rows, :] = (attended * scale * gain_ref[...]).astype(jnp.bfloat16)


def finish(order, near, far, carried, gain, n_p, n_tp):
    rows = near.shape[0] // (n_p * n_tp)
    return pl.pallas_call(
        finish_kernel,
        grid_spec=pltpu.PrefetchScalarGridSpec(
            num_scalar_prefetch=1,
            grid=(n_tp,),
            in_specs=[
                pl.BlockSpec((n_p, 1, rows, DV), lambda i, order: (0, order[i], 0, 0)),
                pl.BlockSpec((n_p, 1, rows, DK), lambda i, order: (0, order[i], 0, 0)),
                pl.BlockSpec((DK, DV), lambda i, order: (0, 0)),
                pl.BlockSpec((1, DV), lambda i, order: (0, 0)),
            ],
            out_specs=pl.BlockSpec((1, n_p * rows, DV), lambda i, order: (i, 0, 0)),
        ),
        out_shape=jax.ShapeDtypeStruct((n_tp, n_p * rows, DV), jnp.bfloat16),
        name="finish",
    )(order, near.reshape(n_p, n_tp, rows, DV), far.reshape(n_p, n_tp, rows, DK), carried, gain.reshape(1, DV))


def entering(state, total, n_sp, n_p):
    n_z = n_sp // n_p
    if n_z > SHORT:
        step = 1
        while step < n_z:
            pairs = [(s, s + step * n_p) for s in range(n_sp - step * n_p)]
            state, total = (
                state + jnp.exp(total)[:, None] * lax.ppermute(state, "sp", pairs),
                total + lax.ppermute(total, "sp", pairs),
            )
            step *= 2
        return lax.ppermute(state, "sp", [(s, s + n_p) for s in range(n_sp - n_p)])
    sent = state.astype(jnp.bfloat16)
    result = jnp.zeros(state.shape, jnp.float32)
    since = jnp.zeros(total.shape, jnp.float32)
    for step in range(1, n_z):
        pairs = [(s, s + step * n_p) for s in range(n_sp - step * n_p)]
        far, decay = lax.ppermute(sent, "sp", pairs), lax.ppermute(total, "sp", pairs)
        result = result + jnp.exp(since)[:, None] * far.astype(jnp.float32)
        since = since + decay
    return result


def on_device(
    tokens,
    norm_gain,
    w_query,
    w_key,
    w_value,
    w_rank_down,
    w_rank_up,
    gate_bias,
    decay_shift,
    out_gain,
    w_out,
):
    n_sp, n_tp = lax.axis_size("sp"), lax.axis_size("tp")
    sp, tp = lax.axis_index("sp"), lax.axis_index("tp")
    n_p = w_query.shape[1] // DK
    n_z = n_sp // n_p
    p, z = sp % n_p, sp // n_p
    width = tokens.shape[1]
    groups = [[i * n_p + j for j in range(n_p)] for i in range(n_z)]

    def plane_of(step):
        return plane_pairs(n_sp, n_p, step) if step else None

    def core_of(step):
        return [(t, partner(t, step, n_tp)) for t in range(n_tp)] if step else None

    def exchange(value):
        if n_p == 1:
            return value
        return lax.all_to_all(value, "sp", 0, 0, axis_index_groups=groups, tiled=True)

    rows = w_query.shape[0]
    short = n_z <= SHORT
    out_rows = w_out.shape[0] // n_p
    raw = w_out.reshape(n_p, out_rows, w_out.shape[1])
    up_z = [(s, (s + n_p) % n_sp) for s in range(n_sp)]
    if short and n_z > 1:
        raw_next = lax.ppermute(raw, "sp", up_z)
    packed = pack(w_query, w_key, w_value)
    weights = exchange(packed).reshape(n_p * rows, 2 * DK + DV)
    if short:
        depth = n_p * rows
        weights = [weights]
        for _ in range(1, n_z):
            weights.append(lax.ppermute(weights[-1], "sp", up_z))
        outs = [exchange(raw)]
        if n_z > 1:
            outs.append(exchange(raw_next))
        for _ in range(2, n_z):
            outs.append(lax.ppermute(outs[-1], "sp", up_z))
        wide = jnp.zeros((out_rows, width), jnp.bfloat16)
        for step, block in enumerate(outs):
            block = block.transpose(1, 0, 2).reshape(out_rows, width // n_z)
            wide = lax.dynamic_update_slice_in_dim(wide, block, (z - step) % n_z * (width // n_z), axis=1)
    else:
        depth = n_sp * rows
        weights = [gather_planes(weights, n_sp, n_p).reshape(depth, 2 * DK + DV)]
        wide = gather_planes(exchange(raw), n_sp, n_p).reshape(n_sp, out_rows, w_out.shape[1])
        wide = wide.transpose(1, 0, 2).reshape(out_rows, width)

    normed = rms_rows(tokens, norm_gain).astype(jnp.bfloat16)
    plane = gather_blocks(normed, "sp", p, n_p, plane_of)
    whole = gather_blocks(plane, "tp", tp, n_tp, core_of)
    span = n_p * n_tp * tokens.shape[0]
    whole = whole.transpose(1, 0, 2, 3).reshape(span, width)
    shift = gather_blocks(decay_shift, "sp", p, n_p, plane_of).reshape(span)

    rank = jnp.dot(whole, w_rank_down, preferred_element_type=jnp.float32).astype(jnp.bfloat16)
    up = lax.dynamic_slice_in_dim(w_rank_up, p * DK, DK, axis=1)
    bias = lax.dynamic_slice_in_dim(gate_bias, p * DK, DK, axis=0)
    pre = jnp.dot(rank, up, preferred_element_type=jnp.float32) + bias
    log_decay = jax.nn.log_sigmoid(pre) / TAU + shift[:, None]
    cumul = jnp.cumsum(log_decay.reshape(span // BLOCK, BLOCK, DK), axis=1)
    final = cumul[:, -1]
    upto = jnp.cumsum(final, axis=0)
    before, total = upto - final, upto[-1]
    to_end = jnp.exp(total - before[:, None] - cumul).reshape(span, DK)
    cumul = cumul.reshape(span, DK)

    joined = jnp.zeros((span, 2 * DK + DV), jnp.float32)
    for step, block in enumerate(weights):
        part = lax.dynamic_slice_in_dim(whole, (z - step) % n_z * depth if short else 0, depth, axis=1)
        joined = joined + jnp.dot(part, block, preferred_element_type=jnp.float32)
    joined = joined.astype(jnp.bfloat16)

    last_k = (joined[:, DK : 2 * DK].astype(jnp.float32) * to_end).astype(jnp.bfloat16)
    state = jnp.einsum("td,te->de", last_k, joined[:, 2 * DK :], preferred_element_type=jnp.float32)
    carried = entering(state, total, n_sp, n_p).astype(jnp.bfloat16)
    near, far = attend(joined, cumul, before)
    order = jnp.stack([partner(tp, step, n_tp) if step else tp for step in range(n_tp)]).astype(jnp.int32)
    shaped = finish(order, near, far, carried, out_gain, n_p, n_tp)

    parts = []
    for cut in range(CUTS):
        columns = wide[:, cut * (width // CUTS) : (cut + 1) * (width // CUTS)]
        sent = [
            lax.ppermute(
                jnp.dot(shaped[step], columns, preferred_element_type=jnp.float32).astype(jnp.bfloat16),
                "tp",
                core_of(step),
            )
            for step in range(1, n_tp)
        ]
        mine = jnp.dot(shaped[0], columns, preferred_element_type=jnp.float32)
        for part in sent:
            mine = mine + part.astype(jnp.float32)
        mine = mine.astype(jnp.bfloat16).reshape(n_p, tokens.shape[0], width // CUTS)
        here = lax.dynamic_index_in_dim(mine, p, 0, keepdims=False).astype(jnp.float32)
        for step in range(1, n_p):
            part = lax.dynamic_index_in_dim(mine, partner(p, step, n_p), 0, keepdims=False)
            here = here + lax.ppermute(part, "sp", plane_of(step)).astype(jnp.float32)
        parts.append(here.astype(jnp.bfloat16))
    return jnp.concatenate(parts, axis=1)


def solution(mesh):
    return jax.shard_map(
        on_device,
        mesh=mesh,
        in_specs=(
            P(("sp", "tp"), None),
            P(),
            P("sp", "tp"),
            P("sp", "tp"),
            P("sp", "tp"),
            P(),
            P(None, "tp"),
            P("tp"),
            P("sp"),
            P(),
            P("tp", "sp"),
        ),
        out_specs=P(("sp", "tp"), None),
        check_vma=False,
    )
```

```python
import functools

import jax
import jax.numpy as jnp
from jax import lax
from jax.experimental import pallas as pl
from jax.experimental.pallas import tpu as pltpu
from jax.sharding import PartitionSpec as P


DK = 256
DV = 512
TAU = 16
BLOCK = 64
EPS = 1e-06
SHORT = 8


def rms_rows(values, gain):
    wide = values.astype(jnp.float32)
    return wide * lax.rsqrt(jnp.mean(wide * wide, axis=-1, keepdims=True) + EPS) * gain


def partner(index, step, count):
    if count & (count - 1) == 0:
        return index ^ step
    return (step - index) % count


def plane_pairs(n_sp, n_p, step):
    return [(s, s // n_p * n_p + partner(s % n_p, step, n_p)) for s in range(n_sp)]


def gather_blocks(value, axis, index, count, pairs_of):
    out = jnp.zeros((count,) + value.shape, value.dtype)
    for step in range(count):
        got = value if pairs_of(step) is None else lax.ppermute(value, axis, pairs_of(step))
        out = lax.dynamic_update_index_in_dim(out, got, partner(index, step, count), 0)
    return out


def gather_planes(value, n_sp, n_p):
    lines = [[i + j * n_p for j in range(n_sp // n_p)] for i in range(n_p)]
    return lax.all_gather(value, "sp", axis_index_groups=lines)


def pack_kernel(q_ref, k_ref, v_ref, out_ref):
    out_ref[0, :, :DK] = q_ref[...]
    out_ref[0, :, DK : 2 * DK] = k_ref[...]
    out_ref[0, :, 2 * DK :] = v_ref[...]


def pack(w_query, w_key, w_value):
    rows = w_query.shape[0]
    heads = w_query.shape[1] // DK
    return pl.pallas_call(
        pack_kernel,
        grid=(heads,),
        in_specs=[
            pl.BlockSpec((rows, DK), lambda h: (0, h)),
            pl.BlockSpec((rows, DK), lambda h: (0, h)),
            pl.BlockSpec((rows, DV), lambda h: (0, h)),
        ],
        out_specs=pl.BlockSpec((1, rows, 2 * DK + DV), lambda h: (h, 0, 0)),
        out_shape=jax.ShapeDtypeStruct((heads, rows, 2 * DK + DV), jnp.bfloat16),
        compiler_params=pltpu.CompilerParams(vmem_limit_bytes=4 << 20),
        name="pack",
    )(w_query, w_key, w_value)


def mm(left, right, dims):
    return lax.dot_general(left, right, (dims, ((), ())), preferred_element_type=jnp.float32)


def decays_kernel(pre_ref, shift_ref, cumul_ref, before_ref, to_end_ref, decay_ref):
    blocks = pre_ref.shape[0] // BLOCK
    row = lax.broadcasted_iota(jnp.int32, (BLOCK, BLOCK), 0)
    column = lax.broadcasted_iota(jnp.int32, (BLOCK, BLOCK), 1)
    lower = jnp.where(row >= column, 1.0, 0.0).astype(jnp.float32)
    upto = jnp.zeros((1, pre_ref.shape[1]), jnp.float32)
    for n in range(blocks):
        span = slice(n * BLOCK, (n + 1) * BLOCK)
        log_decay = jax.nn.log_sigmoid(pre_ref[span, :]) / TAU + shift_ref[span, :]
        cumul = lax.dot_general(
            lower,
            log_decay,
            (((1,), (0,)), ((), ())),
            precision=lax.Precision.HIGHEST,
            preferred_element_type=jnp.float32,
        )
        cumul_ref[span, :] = cumul
        before_ref[n : n + 1, :] = upto
        upto = upto + cumul[BLOCK - 1 :, :]
    decay_ref[...] = jnp.exp(upto)
    for n in range(blocks):
        span = slice(n * BLOCK, (n + 1) * BLOCK)
        to_end_ref[span, :] = jnp.exp((upto - before_ref[n : n + 1, :]) - cumul_ref[span, :])


def decays(pre, shift):
    rows, width = pre.shape
    return pl.pallas_call(
        decays_kernel,
        out_shape=(
            jax.ShapeDtypeStruct((rows, width), jnp.float32),
            jax.ShapeDtypeStruct((rows // BLOCK, width), jnp.float32),
            jax.ShapeDtypeStruct((rows, width), jnp.float32),
            jax.ShapeDtypeStruct((1, width), jnp.float32),
        ),
        compiler_params=pltpu.CompilerParams(vmem_limit_bytes=12 << 20),
        cost_estimate=pl.CostEstimate(flops=1_000_000_000, transcendentals=1_000_000, bytes_accessed=4_000_000),
        name="decays",
    )(pre, shift.reshape(rows, 1))


def project_kernel(index_ref, *refs, count, started):
    parts, blocks, out_ref = refs[:count], refs[count : 2 * count], refs[-1]
    total = sum(mm(x[...], w[...], ((1,), (0,))) for x, w in zip(parts, blocks))
    out_ref[...] = total + refs[2 * count][...] if started else total


def project(index, whole, blocks, total):
    rows, (depth, width), count = whole.shape[0], blocks[0].shape, len(blocks)
    tile = min(rows, 256)

    def part_spec(i):
        return pl.BlockSpec((tile, depth), lambda m, index: (m, index[i]))

    started = total is not None
    return pl.pallas_call(
        functools.partial(project_kernel, count=count, started=started),
        grid_spec=pltpu.PrefetchScalarGridSpec(
            num_scalar_prefetch=1,
            grid=(rows // tile,),
            in_specs=[part_spec(i) for i in range(count)]
            + [pl.BlockSpec((depth, width), lambda m, index: (0, 0))] * count
            + [pl.BlockSpec((tile, width), lambda m, index: (m, 0))] * started,
            out_specs=pl.BlockSpec((tile, width), lambda m, index: (m, 0)),
        ),
        out_shape=jax.ShapeDtypeStruct((rows, width), jnp.float32),
        compiler_params=pltpu.CompilerParams(vmem_limit_bytes=20 << 20),
        cost_estimate=pl.CostEstimate(
            flops=2 * rows * depth * width * count, transcendentals=0, bytes_accessed=8 * rows * width
        ),
        name="project",
    )(index, *([whole] * count), *blocks, *([total] if started else []))


def close_kernel(index_ref, part_ref, block_ref, *refs, started):
    to_end_ref, joined_ref, state_ref, held = refs[-4:]
    total = mm(part_ref[...], block_ref[...], ((1,), (0,)))
    if started:
        total = total + refs[0][...]
    joined = total.astype(jnp.bfloat16)
    joined_ref[...] = joined
    last_k = (joined[:, DK : 2 * DK].astype(jnp.float32) * to_end_ref[...]).astype(jnp.bfloat16)
    added = mm(last_k, joined[:, 2 * DK :], ((0,), (0,)))
    step = pl.program_id(0)

    @pl.when(step == 0)
    def _():
        held[...] = added

    @pl.when(step > 0)
    def _():
        held[...] += added

    state_ref[...] = held[...]


def close(index, whole, block, total, to_end):
    rows, (depth, width) = whole.shape[0], block.shape
    tile = min(rows, 256)
    started = total is not None
    return pl.pallas_call(
        functools.partial(close_kernel, started=started),
        grid_spec=pltpu.PrefetchScalarGridSpec(
            num_scalar_prefetch=1,
            grid=(rows // tile,),
            in_specs=[
                pl.BlockSpec((tile, depth), lambda m, index: (m, index[0])),
                pl.BlockSpec((depth, width), lambda m, index: (0, 0)),
            ]
            + [pl.BlockSpec((tile, width), lambda m, index: (m, 0))] * started
            + [pl.BlockSpec((tile, DK), lambda m, index: (m, 0))],
            out_specs=[
                pl.BlockSpec((tile, width), lambda m, index: (m, 0)),
                pl.BlockSpec((DK, DV), lambda m, index: (0, 0)),
            ],
            scratch_shapes=[pltpu.VMEM((DK, DV), jnp.float32)],
        ),
        out_shape=(
            jax.ShapeDtypeStruct((rows, width), jnp.bfloat16),
            jax.ShapeDtypeStruct((DK, DV), jnp.float32),
        ),
        compiler_params=pltpu.CompilerParams(vmem_limit_bytes=24 << 20),
        cost_estimate=pl.CostEstimate(
            flops=2 * rows * depth * width, transcendentals=0, bytes_accessed=8 * rows * width
        ),
        name="close",
    )(index, whole, block, *([total] if started else []), to_end)


def reduce_plane(mine, p, n_sp, n_p, flip):
    bits = [1 << i for i in range(n_p.bit_length() - 1)]
    if n_p != 1 << len(bits):
        here = lax.dynamic_index_in_dim(mine, p, 0, keepdims=False).astype(jnp.float32)
        for step in range(1, n_p):
            part = lax.dynamic_index_in_dim(mine, partner(p, step, n_p), 0, keepdims=False)
            here = here + lax.ppermute(part, "sp", plane_pairs(n_sp, n_p, step)).astype(jnp.float32)
        return here.astype(jnp.bfloat16)
    mine = mine.reshape((2,) * len(bits) + mine.shape[1:])
    left = list(reversed(bits))
    for bit in bits if flip else left[:]:
        axis = left.index(bit)
        side = p // bit % 2
        keep = lax.dynamic_index_in_dim(mine, side, axis, keepdims=False)
        give = lax.dynamic_index_in_dim(mine, 1 - side, axis, keepdims=False)
        got = lax.ppermute(give, "sp", plane_pairs(n_sp, n_p, bit))
        mine = (keep.astype(jnp.float32) + got.astype(jnp.float32)).astype(jnp.bfloat16)
        left.remove(bit)
    return mine


def attend_kernel(joined_ref, cumul_ref, before_ref, near_ref, far_ref, state_ref):
    blocks = joined_ref.shape[0] // BLOCK
    row = lax.broadcasted_iota(jnp.int32, (BLOCK, BLOCK), 0)
    column = lax.broadcasted_iota(jnp.int32, (BLOCK, BLOCK), 1)
    for n in range(blocks):
        span = slice(n * BLOCK, (n + 1) * BLOCK)
        q = joined_ref[span, :DK].astype(jnp.float32) * DK ** (-0.5)
        k = joined_ref[span, DK : 2 * DK].astype(jnp.float32)
        v = joined_ref[span, 2 * DK :]
        cumul = cumul_ref[span, :]
        centre = cumul - cumul[BLOCK // 2 : BLOCK // 2 + 1, :]
        final = cumul[BLOCK - 1 :, :]
        q_scaled = (q * jnp.exp(centre)).astype(jnp.bfloat16)
        k_scaled = (k * jnp.exp(-centre)).astype(jnp.bfloat16)
        scores = mm(q_scaled, k_scaled, ((1,), (1,)))
        scores = jnp.where(row >= column, scores, 0.0).astype(jnp.bfloat16)
        near = mm(scores, v, ((1,), (0,)))
        reach = q * jnp.exp(cumul)
        if n:
            near = near + mm(reach.astype(jnp.bfloat16), state_ref[...].astype(jnp.bfloat16), ((1,), (1,)))
        near_ref[span, :] = near
        far_ref[span, :] = (reach * jnp.exp(before_ref[n : n + 1, :])).astype(jnp.bfloat16)
        if n < blocks - 1:
            decayed = (k * jnp.exp(final - cumul)).astype(jnp.bfloat16)
            added = mm(v, decayed, ((0,), (0,)))
            state_ref[...] = state_ref[...] * jnp.exp(final) + added if n else added


def attend(joined, cumul, before):
    rows = joined.shape[0]
    return pl.pallas_call(
        attend_kernel,
        out_shape=(
            jax.ShapeDtypeStruct((rows, DV), jnp.float32),
            jax.ShapeDtypeStruct((rows, DK), jnp.bfloat16),
        ),
        scratch_shapes=[pltpu.VMEM((DV, DK), jnp.float32)],
        compiler_params=pltpu.CompilerParams(vmem_limit_bytes=12 << 20),
        cost_estimate=pl.CostEstimate(flops=5_000_000_000, transcendentals=2_000_000, bytes_accessed=6_000_000),
        name="attend",
    )(joined, cumul, before)


def finish_kernel(index_ref, near_ref, far_ref, carried_ref, gain_ref, out_ref):
    parts, rows = near_ref.shape[0], near_ref.shape[2]
    for i in range(parts):
        attended = near_ref[i, 0] + mm(far_ref[i, 0], carried_ref[...], ((1,), (0,)))
        scale = lax.rsqrt(jnp.mean(attended * attended, axis=-1, keepdims=True) + EPS)
        out_ref[0, i * rows : (i + 1) * rows, :] = (attended * scale * gain_ref[...]).astype(jnp.bfloat16)


def finish(order, near, far, carried, gain, n_p, n_tp):
    rows = near.shape[0] // (n_p * n_tp)
    return pl.pallas_call(
        finish_kernel,
        grid_spec=pltpu.PrefetchScalarGridSpec(
            num_scalar_prefetch=1,
            grid=(n_tp,),
            in_specs=[
                pl.BlockSpec((n_p, 1, rows, DV), lambda i, order: (0, order[i], 0, 0)),
                pl.BlockSpec((n_p, 1, rows, DK), lambda i, order: (0, order[i], 0, 0)),
                pl.BlockSpec((DK, DV), lambda i, order: (0, 0)),
                pl.BlockSpec((1, DV), lambda i, order: (0, 0)),
            ],
            out_specs=pl.BlockSpec((1, n_p * rows, DV), lambda i, order: (i, 0, 0)),
        ),
        out_shape=jax.ShapeDtypeStruct((n_tp, n_p * rows, DV), jnp.bfloat16),
        compiler_params=pltpu.CompilerParams(vmem_limit_bytes=12 << 20),
        name="finish",
    )(order, near.reshape(n_p, n_tp, rows, DV), far.reshape(n_p, n_tp, rows, DK), carried, gain.reshape(1, DV))


def entering(state, decay, n_sp, n_p):
    n_z = n_sp // n_p
    if n_z > SHORT:
        step = 1
        while step < n_z:
            pairs = [(s, s + step * n_p) for s in range(n_sp - step * n_p)]
            have = lax.axis_index("sp") >= step * n_p
            state, decay = (
                state + decay[:, None] * lax.ppermute(state, "sp", pairs),
                decay * jnp.where(have, lax.ppermute(decay, "sp", pairs), 1.0),
            )
            step *= 2
        return lax.ppermute(state, "sp", [(s, s + n_p) for s in range(n_sp - n_p)])
    result = jnp.zeros(state.shape, jnp.float32)
    passed = jnp.ones(decay.shape, jnp.float32)
    step = 1
    while step < n_z:
        pairs = [(s, s + step * n_p) for s in range(n_sp - step * n_p)]
        got = lax.ppermute(state.astype(jnp.bfloat16), "sp", pairs).astype(jnp.float32)
        far = lax.ppermute(decay, "sp", pairs)
        result = result + passed[:, None] * got
        if 2 * step < n_z:
            state = state + decay[:, None] * got
            passed = passed * far
            decay = decay * far
        step *= 2
    return result


def on_device(
    tokens,
    norm_gain,
    w_query,
    w_key,
    w_value,
    w_rank_down,
    w_rank_up,
    gate_bias,
    decay_shift,
    out_gain,
    w_out,
):
    n_sp, n_tp = lax.axis_size("sp"), lax.axis_size("tp")
    sp, tp = lax.axis_index("sp"), lax.axis_index("tp")
    n_p = w_query.shape[1] // DK
    n_z = n_sp // n_p
    p, z = sp % n_p, sp // n_p
    width = tokens.shape[1]
    groups = [[i * n_p + j for j in range(n_p)] for i in range(n_z)]

    def plane_of(step):
        return plane_pairs(n_sp, n_p, step) if step else None

    def core_of(step):
        return [(t, partner(t, step, n_tp)) for t in range(n_tp)] if step else None

    def exchange(value):
        if n_p == 1:
            return value
        return lax.all_to_all(value, "sp", 0, 0, axis_index_groups=groups, tiled=True)

    rows = w_query.shape[0]
    short = n_z <= SHORT
    out_rows = w_out.shape[0] // n_p
    raw = w_out.reshape(n_p, out_rows, w_out.shape[1])
    up_z = [(s, (s + n_p) % n_sp) for s in range(n_sp)]
    if short and n_z > 1:
        raw_next = lax.ppermute(raw, "sp", up_z)
    packed = pack(w_query, w_key, w_value)
    weights = exchange(packed).reshape(n_p * rows, 2 * DK + DV)
    if short:
        depth = n_p * rows
        weights = [weights]
        for _ in range(1, n_z):
            weights.append(lax.ppermute(weights[-1], "sp", up_z))
        first = [raw] if n_z == 1 else [raw, raw_next]
        first = exchange(jnp.stack(first, axis=1))
        outs = [first[:, i] for i in range(first.shape[1])]
        for _ in range(2, n_z):
            outs.append(lax.ppermute(outs[-1], "sp", up_z))
        outs = [block.transpose(1, 0, 2).reshape(out_rows, width // n_z) for block in outs]
        half = (n_z + 1) // 2
        cuts = [jnp.concatenate(group, axis=1) for group in (outs[:half], outs[half:]) if group]
    else:
        depth = n_sp * rows
        weights = [gather_planes(weights, n_sp, n_p).reshape(depth, 2 * DK + DV)]
        wide = gather_planes(exchange(raw), n_sp, n_p).reshape(n_sp, out_rows, w_out.shape[1])
        cuts = [wide.transpose(1, 0, 2).reshape(out_rows, width)]

    normed = rms_rows(tokens, norm_gain).astype(jnp.bfloat16)
    plane = gather_blocks(normed, "sp", p, n_p, plane_of)
    whole = gather_blocks(plane, "tp", tp, n_tp, core_of)
    span = n_p * n_tp * tokens.shape[0]
    whole = whole.transpose(1, 0, 2, 3).reshape(span, width)
    shift = gather_blocks(decay_shift, "sp", p, n_p, plane_of).reshape(span)

    rank = jnp.dot(whole, w_rank_down, preferred_element_type=jnp.float32).astype(jnp.bfloat16)
    up = lax.dynamic_slice_in_dim(w_rank_up, p * DK, DK, axis=1)
    bias = lax.dynamic_slice_in_dim(gate_bias, p * DK, DK, axis=0)
    pre = jnp.dot(rank, up, preferred_element_type=jnp.float32) + bias
    cumul, before, to_end, decay = decays(pre, shift)

    owners = ((z - jnp.arange(n_z)) % n_z if short else jnp.zeros(1, jnp.int32)).astype(jnp.int32)
    total, early = None, max(len(weights) - 2, 0)
    if early:
        total = project(owners[:early], whole, weights[:early], None)
    if len(weights) > 1:
        total = project(owners[early : early + 1], whole, weights[early : early + 1], total)
    joined, state = close(owners[-1:], whole, weights[-1], total, to_end)
    carried = entering(state, decay[0], n_sp, n_p).astype(jnp.bfloat16)
    near, far = attend(joined, cumul, before)
    order = jnp.stack([partner(tp, step, n_tp) if step else tp for step in range(n_tp)]).astype(jnp.int32)
    shaped = finish(order, near, far, carried, out_gain, n_p, n_tp)

    parts = []
    for columns in cuts:
        sent = [
            lax.ppermute(
                jnp.dot(shaped[step], columns, preferred_element_type=jnp.float32).astype(jnp.bfloat16),
                "tp",
                core_of(step),
            )
            for step in range(1, n_tp)
        ]
        mine = jnp.dot(shaped[0], columns, preferred_element_type=jnp.float32)
        for part in sent:
            mine = mine + part.astype(jnp.float32)
        mine = mine.astype(jnp.bfloat16).reshape(n_p, tokens.shape[0], columns.shape[1])
        parts.append(reduce_plane(mine, p, n_sp, n_p, len(parts) % 2))
    if not short:
        return parts[0]
    mixed = jnp.zeros(tokens.shape, jnp.bfloat16)
    block = width // n_z
    for step in range(n_z):
        part = parts[step // half][:, step % half * block : (step % half + 1) * block]
        mixed = lax.dynamic_update_slice_in_dim(mixed, part, (z - step) % n_z * block, axis=1)
    return mixed


def solution(mesh):
    return jax.shard_map(
        on_device,
        mesh=mesh,
        in_specs=(
            P(("sp", "tp"), None),
            P(),
            P("sp", "tp"),
            P("sp", "tp"),
            P("sp", "tp"),
            P(),
            P(None, "tp"),
            P("tp"),
            P("sp"),
            P(),
            P("tp", "sp"),
        ),
        out_specs=P(("sp", "tp"), None),
        check_vma=False,
    )
```

```python
import functools

import jax
import jax.numpy as jnp
from jax import lax
from jax.experimental import pallas as pl
from jax.experimental.pallas import tpu as pltpu
from jax.sharding import PartitionSpec as P


DK = 256
DV = 512
TAU = 16
BLOCK = 64
EPS = 1e-06
SHORT = 8


def partner(index, step, count):
    if count & (count - 1) == 0:
        return index ^ step
    return (step - index) % count


def plane_pairs(n_sp, n_p, step):
    return [(s, s // n_p * n_p + partner(s % n_p, step, n_p)) for s in range(n_sp)]


def gather_blocks(value, axis, index, count, pairs_of):
    values = value if isinstance(value, (list, tuple)) else [value] * count
    out = jnp.zeros((count,) + values[0].shape, values[0].dtype)
    out = lax.dynamic_update_index_in_dim(out, values[0], index, 0)
    for step in range(1, count):
        got = lax.ppermute(values[step], axis, pairs_of(step))
        out = lax.dynamic_update_index_in_dim(out, got, partner(index, step, count), 0)
    return out


def line(own, ahead, n_sp, n_p):
    n_z = n_sp // n_p
    up = [(s, (s + n_p) % n_sp) for s in range(n_sp)]
    down = [(s, (s - n_p) % n_sp) for s in range(n_sp)]
    blocks, offsets = [own], [0]
    if n_z > 1:
        if ahead is None:
            ahead = lax.ppermute(own, "sp", up)
        blocks.append(ahead)
        offsets.append(1)
    if n_z > 2:
        blocks.append(lax.ppermute(own, "sp", down))
        offsets.append(n_z - 1)
    for offset in range(2, n_z - 1):
        ahead = lax.ppermute(ahead, "sp", up)
        blocks.append(ahead)
        offsets.append(offset)
    return blocks, offsets


def gather_planes(value, n_sp, n_p):
    lines = [[i + j * n_p for j in range(n_sp // n_p)] for i in range(n_p)]
    return lax.all_gather(value, "sp", axis_index_groups=lines)


def pack_kernel(order_ref, q_ref, k_ref, v_ref, *out_refs):
    for i, out_ref in enumerate(out_refs):
        head = order_ref[i]
        narrow = pl.ds(pl.multiple_of(head * DK, DK), DK)
        wide = pl.ds(pl.multiple_of(head * DV, DV), DV)
        out_ref[:, :DK] = q_ref[:, narrow]
        out_ref[:, DK : 2 * DK] = k_ref[:, narrow]
        out_ref[:, 2 * DK :] = v_ref[:, wide]


def whole_specs(count):
    return [pl.BlockSpec(memory_space=pltpu.VMEM)] * count


def pack(order, w_query, w_key, w_value):
    rows = w_query.shape[0]
    heads = w_query.shape[1] // DK
    return pl.pallas_call(
        pack_kernel,
        in_specs=[pl.BlockSpec(memory_space=pltpu.SMEM)] + whole_specs(3),
        out_specs=whole_specs(heads),
        out_shape=[jax.ShapeDtypeStruct((rows, 2 * DK + DV), jnp.bfloat16)] * heads,
        compiler_params=pltpu.CompilerParams(vmem_limit_bytes=8 << 20),
        name="pack",
    )(order, w_query, w_key, w_value)


def norm_kernel(order_ref, tokens_ref, gain_ref, *refs, rows):
    out_refs, held = refs[:-1], refs[-1]
    wide = tokens_ref[...].astype(jnp.float32)
    scale = lax.rsqrt(jnp.mean(wide * wide, axis=-1, keepdims=True) + EPS)
    held[...] = (wide * scale * gain_ref[...]).astype(jnp.bfloat16)
    count = len(out_refs)
    if count == 1:
        out_refs[0][...] = held[...]
        return
    for i, out_ref in enumerate(out_refs):
        for block in range(held.shape[1] // rows):
            base, j = block // count * count, block % count
            source = base + order_ref[i * count + j]
            out_ref[:, block * rows : (block + 1) * rows] = held[:, pl.ds(pl.multiple_of(source * rows, rows), rows)]


def norm(order, tokens, gain, rows, count):
    return pl.pallas_call(
        functools.partial(norm_kernel, rows=rows),
        in_specs=[pl.BlockSpec(memory_space=pltpu.SMEM)] + whole_specs(2),
        out_specs=whole_specs(count),
        out_shape=[jax.ShapeDtypeStruct(tokens.shape, jnp.bfloat16)] * count,
        scratch_shapes=[pltpu.VMEM(tokens.shape, jnp.bfloat16)],
        compiler_params=pltpu.CompilerParams(vmem_limit_bytes=12 << 20),
        name="norm",
    )(order, tokens, gain.reshape(1, -1))


def mm(left, right, dims):
    return lax.dot_general(left, right, (dims, ((), ())), preferred_element_type=jnp.float32)


def decays_kernel(pre_ref, shift_ref, cumul_ref, before_ref, to_end_ref, decay_ref):
    blocks = pre_ref.shape[0] // BLOCK
    row = lax.broadcasted_iota(jnp.int32, (BLOCK, BLOCK), 0)
    column = lax.broadcasted_iota(jnp.int32, (BLOCK, BLOCK), 1)
    lower = jnp.where(row >= column, 1.0, 0.0).astype(jnp.float32)
    upto = jnp.zeros((1, pre_ref.shape[1]), jnp.float32)
    for n in range(blocks):
        span = slice(n * BLOCK, (n + 1) * BLOCK)
        log_decay = jax.nn.log_sigmoid(pre_ref[span, :]) / TAU + shift_ref[span, :]
        cumul = lax.dot_general(
            lower,
            log_decay,
            (((1,), (0,)), ((), ())),
            precision=lax.Precision.HIGHEST,
            preferred_element_type=jnp.float32,
        )
        cumul_ref[span, :] = cumul
        before_ref[n : n + 1, :] = upto
        upto = upto + cumul[BLOCK - 1 :, :]
    decay_ref[...] = jnp.exp(upto)
    for n in range(blocks):
        span = slice(n * BLOCK, (n + 1) * BLOCK)
        to_end_ref[span, :] = jnp.exp((upto - before_ref[n : n + 1, :]) - cumul_ref[span, :])


def decays(pre, shift):
    rows, width = pre.shape
    return pl.pallas_call(
        decays_kernel,
        out_shape=(
            jax.ShapeDtypeStruct((rows, width), jnp.float32),
            jax.ShapeDtypeStruct((rows // BLOCK, width), jnp.float32),
            jax.ShapeDtypeStruct((rows, width), jnp.float32),
            jax.ShapeDtypeStruct((1, width), jnp.float32),
        ),
        compiler_params=pltpu.CompilerParams(vmem_limit_bytes=12 << 20),
        cost_estimate=pl.CostEstimate(flops=1_000_000_000, transcendentals=1_000_000, bytes_accessed=4_000_000),
        name="decays",
    )(pre, shift.reshape(rows, 1))


def project_kernel(index_ref, *refs, count, started):
    parts, blocks, out_ref = refs[:count], refs[count : 2 * count], refs[-1]
    total = sum(mm(x[...], w[...], ((1,), (0,))) for x, w in zip(parts, blocks))
    out_ref[...] = total + refs[2 * count][...] if started else total


def project(index, whole, blocks, total):
    rows, (depth, width), count = whole.shape[0], blocks[0].shape, len(blocks)
    tile = min(rows, 256)

    def part_spec(i):
        return pl.BlockSpec((tile, depth), lambda m, index: (m, index[i]))

    started = total is not None
    return pl.pallas_call(
        functools.partial(project_kernel, count=count, started=started),
        grid_spec=pltpu.PrefetchScalarGridSpec(
            num_scalar_prefetch=1,
            grid=(rows // tile,),
            in_specs=[part_spec(i) for i in range(count)]
            + [pl.BlockSpec((depth, width), lambda m, index: (0, 0))] * count
            + [pl.BlockSpec((tile, width), lambda m, index: (m, 0))] * started,
            out_specs=pl.BlockSpec((tile, width), lambda m, index: (m, 0)),
        ),
        out_shape=jax.ShapeDtypeStruct((rows, width), jnp.float32),
        compiler_params=pltpu.CompilerParams(vmem_limit_bytes=20 << 20),
        cost_estimate=pl.CostEstimate(
            flops=2 * rows * depth * width * count, transcendentals=0, bytes_accessed=8 * rows * width
        ),
        name="project",
    )(index, *([whole] * count), *blocks, *([total] if started else []))


def close_kernel(index_ref, part_ref, block_ref, *refs, started):
    to_end_ref, joined_ref, state_ref, held = refs[-4:]
    total = mm(part_ref[...], block_ref[...], ((1,), (0,)))
    if started:
        total = total + refs[0][...]
    joined = total.astype(jnp.bfloat16)
    joined_ref[...] = joined
    last_k = (joined[:, DK : 2 * DK].astype(jnp.float32) * to_end_ref[...]).astype(jnp.bfloat16)
    added = mm(last_k, joined[:, 2 * DK :], ((0,), (0,)))
    step = pl.program_id(0)

    @pl.when(step == 0)
    def _():
        held[...] = added

    @pl.when(step > 0)
    def _():
        held[...] += added

    state_ref[...] = held[...]


def close(index, whole, block, total, to_end):
    rows, (depth, width) = whole.shape[0], block.shape
    tile = min(rows, 256)
    started = total is not None
    return pl.pallas_call(
        functools.partial(close_kernel, started=started),
        grid_spec=pltpu.PrefetchScalarGridSpec(
            num_scalar_prefetch=1,
            grid=(rows // tile,),
            in_specs=[
                pl.BlockSpec((tile, depth), lambda m, index: (m, index[0])),
                pl.BlockSpec((depth, width), lambda m, index: (0, 0)),
            ]
            + [pl.BlockSpec((tile, width), lambda m, index: (m, 0))] * started
            + [pl.BlockSpec((tile, DK), lambda m, index: (m, 0))],
            out_specs=[
                pl.BlockSpec((tile, width), lambda m, index: (m, 0)),
                pl.BlockSpec((DK, DV), lambda m, index: (0, 0)),
            ],
            scratch_shapes=[pltpu.VMEM((DK, DV), jnp.float32)],
        ),
        out_shape=(
            jax.ShapeDtypeStruct((rows, width), jnp.bfloat16),
            jax.ShapeDtypeStruct((DK, DV), jnp.float32),
        ),
        compiler_params=pltpu.CompilerParams(vmem_limit_bytes=24 << 20),
        cost_estimate=pl.CostEstimate(
            flops=2 * rows * depth * width, transcendentals=0, bytes_accessed=8 * rows * width
        ),
        name="close",
    )(index, whole, block, *([total] if started else []), to_end)


def reduce_plane(mine, p, n_sp, n_p, cut):
    bits = [1 << i for i in range(n_p.bit_length() - 1)]
    if n_p != 1 << len(bits):
        here = lax.dynamic_index_in_dim(mine, p, 0, keepdims=False).astype(jnp.float32)
        for step in range(1, n_p):
            part = lax.dynamic_index_in_dim(mine, partner(p, step, n_p), 0, keepdims=False)
            here = here + lax.ppermute(part, "sp", plane_pairs(n_sp, n_p, step)).astype(jnp.float32)
        return here.astype(jnp.bfloat16)
    mine = mine.reshape((2,) * len(bits) + mine.shape[1:])
    left = list(reversed(bits))
    for bit in bits if cut % 2 else left[:]:
        axis = left.index(bit)
        side = p // bit % 2
        keep = lax.dynamic_index_in_dim(mine, side, axis, keepdims=False)
        give = lax.dynamic_index_in_dim(mine, 1 - side, axis, keepdims=False)
        got = lax.ppermute(give, "sp", plane_pairs(n_sp, n_p, bit))
        mine = (keep.astype(jnp.float32) + got.astype(jnp.float32)).astype(jnp.bfloat16)
        left.remove(bit)
    return mine


def attend_kernel(joined_ref, cumul_ref, before_ref, near_ref, far_ref, state_ref):
    blocks = joined_ref.shape[0] // BLOCK
    row = lax.broadcasted_iota(jnp.int32, (BLOCK, BLOCK), 0)
    column = lax.broadcasted_iota(jnp.int32, (BLOCK, BLOCK), 1)
    for n in range(blocks):
        span = slice(n * BLOCK, (n + 1) * BLOCK)
        q = joined_ref[span, :DK].astype(jnp.float32) * DK ** (-0.5)
        k = joined_ref[span, DK : 2 * DK].astype(jnp.float32)
        v = joined_ref[span, 2 * DK :]
        cumul = cumul_ref[span, :]
        centre = cumul - cumul[BLOCK // 2 : BLOCK // 2 + 1, :]
        final = cumul[BLOCK - 1 :, :]
        q_scaled = (q * jnp.exp(centre)).astype(jnp.bfloat16)
        k_scaled = (k * jnp.exp(-centre)).astype(jnp.bfloat16)
        scores = mm(q_scaled, k_scaled, ((1,), (1,)))
        scores = jnp.where(row >= column, scores, 0.0).astype(jnp.bfloat16)
        near = mm(scores, v, ((1,), (0,)))
        reach = q * jnp.exp(cumul)
        if n:
            near = near + mm(reach.astype(jnp.bfloat16), state_ref[...].astype(jnp.bfloat16), ((1,), (1,)))
        near_ref[span, :] = near
        far_ref[span, :] = (reach * jnp.exp(before_ref[n : n + 1, :])).astype(jnp.bfloat16)
        if n < blocks - 1:
            decayed = (k * jnp.exp(final - cumul)).astype(jnp.bfloat16)
            added = mm(v, decayed, ((0,), (0,)))
            state_ref[...] = state_ref[...] * jnp.exp(final) + added if n else added


def attend(joined, cumul, before):
    rows = joined.shape[0]
    return pl.pallas_call(
        attend_kernel,
        out_shape=(
            jax.ShapeDtypeStruct((rows, DV), jnp.float32),
            jax.ShapeDtypeStruct((rows, DK), jnp.bfloat16),
        ),
        scratch_shapes=[pltpu.VMEM((DV, DK), jnp.float32)],
        compiler_params=pltpu.CompilerParams(vmem_limit_bytes=12 << 20),
        cost_estimate=pl.CostEstimate(flops=5_000_000_000, transcendentals=2_000_000, bytes_accessed=6_000_000),
        name="attend",
    )(joined, cumul, before)


def finish_kernel(index_ref, near_ref, far_ref, carried_ref, gain_ref, out_ref):
    parts, rows = near_ref.shape[0], near_ref.shape[2]
    for i in range(parts):
        attended = near_ref[i, 0] + mm(far_ref[i, 0], carried_ref[...], ((1,), (0,)))
        scale = lax.rsqrt(jnp.mean(attended * attended, axis=-1, keepdims=True) + EPS)
        out_ref[0, i * rows : (i + 1) * rows, :] = (attended * scale * gain_ref[...]).astype(jnp.bfloat16)


def finish(order, near, far, carried, gain, n_p, n_tp):
    rows = near.shape[0] // (n_p * n_tp)
    return pl.pallas_call(
        finish_kernel,
        grid_spec=pltpu.PrefetchScalarGridSpec(
            num_scalar_prefetch=1,
            grid=(n_tp,),
            in_specs=[
                pl.BlockSpec((n_p, 1, rows, DV), lambda i, order: (0, order[i], 0, 0)),
                pl.BlockSpec((n_p, 1, rows, DK), lambda i, order: (0, order[i], 0, 0)),
                pl.BlockSpec((DK, DV), lambda i, order: (0, 0)),
                pl.BlockSpec((1, DV), lambda i, order: (0, 0)),
            ],
            out_specs=pl.BlockSpec((1, n_p * rows, DV), lambda i, order: (i, 0, 0)),
        ),
        out_shape=jax.ShapeDtypeStruct((n_tp, n_p * rows, DV), jnp.bfloat16),
        compiler_params=pltpu.CompilerParams(vmem_limit_bytes=12 << 20),
        name="finish",
    )(order, near.reshape(n_p, n_tp, rows, DV), far.reshape(n_p, n_tp, rows, DK), carried, gain.reshape(1, DV))


def entering(state, decay, n_sp, n_p):
    n_z = n_sp // n_p
    if n_z > SHORT:
        step = 1
        while step < n_z:
            pairs = [(s, s + step * n_p) for s in range(n_sp - step * n_p)]
            have = lax.axis_index("sp") >= step * n_p
            state, decay = (
                state + decay[:, None] * lax.ppermute(state, "sp", pairs),
                decay * jnp.where(have, lax.ppermute(decay, "sp", pairs), 1.0),
            )
            step *= 2
        return lax.ppermute(state, "sp", [(s, s + n_p) for s in range(n_sp - n_p)])
    result = jnp.zeros(state.shape, jnp.float32)
    passed = jnp.ones(decay.shape, jnp.float32)
    step = 1
    while step < n_z:
        pairs = [(s, s + step * n_p) for s in range(n_sp - step * n_p)]
        got = lax.ppermute(state.astype(jnp.bfloat16), "sp", pairs).astype(jnp.float32)
        far = lax.ppermute(decay, "sp", pairs)
        result = result + passed[:, None] * got
        if 2 * step < n_z:
            state = state + decay[:, None] * got
            passed = passed * far
            decay = decay * far
        step *= 2
    return result


def on_device(
    tokens,
    norm_gain,
    w_query,
    w_key,
    w_value,
    w_rank_down,
    w_rank_up,
    gate_bias,
    decay_shift,
    out_gain,
    w_out,
):
    n_sp, n_tp = lax.axis_size("sp"), lax.axis_size("tp")
    sp, tp = lax.axis_index("sp"), lax.axis_index("tp")
    n_p = w_query.shape[1] // DK
    n_z = n_sp // n_p
    p, z = sp % n_p, sp // n_p
    width = tokens.shape[1]
    groups = [[i * n_p + j for j in range(n_p)] for i in range(n_z)]

    def plane_of(step):
        return plane_pairs(n_sp, n_p, step) if step else None

    def core_of(step):
        return [(t, partner(t, step, n_tp)) for t in range(n_tp)] if step else None

    def exchange(value):
        if n_p == 1:
            return value
        return lax.all_to_all(value, "sp", 0, 0, axis_index_groups=groups, tiled=True)

    def spread(pieces):
        got = [lax.ppermute(piece, "sp", plane_of(step)) if step else piece for step, piece in enumerate(pieces)]
        return jnp.concatenate(got, axis=0)

    rows = w_query.shape[0]
    others = [partner(p, step, n_p) if step else p for step in range(n_p)]
    heads_order = jnp.stack(others).astype(jnp.int32)
    short = n_z <= SHORT
    out_rows = w_out.shape[0] // n_p
    raw = w_out.reshape(n_p, out_rows, w_out.shape[1])
    if short:
        depth = n_p * rows
        later = None
        if n_z > 1:
            ahead = [(s, (s + n_p) % n_sp) for s in range(n_sp)]
            later = [lax.ppermute(w, "sp", ahead) for w in (w_value, w_key, w_query)]
        own = spread(pack(heads_order, w_query, w_key, w_value))
        if later:
            later = spread(pack(heads_order, *reversed(later)))
            raw, later = lax.optimization_barrier((raw, later))
        weights, offsets = line(own, later, n_sp, n_p)
        own = exchange(raw).transpose(1, 0, 2).reshape(out_rows, width // n_z)
        outs, _ = line(own, None, n_sp, n_p)
        half = (n_z + 1) // 2
        cuts = [jnp.concatenate(outs[:half], axis=1)] + outs[half:]
    else:
        depth, offsets = n_sp * rows, [0]
        packed = spread(pack(heads_order, w_query, w_key, w_value))
        weights = [gather_planes(packed, n_sp, n_p).reshape(depth, 2 * DK + DV)]
        wide = gather_planes(exchange(raw), n_sp, n_p).reshape(n_sp, out_rows, w_out.shape[1])
        cuts = [wide.transpose(1, 0, 2).reshape(out_rows, width)]

    column_order = jnp.stack([partner(other, step, n_p) if step else other for other in others for step in range(n_p)])
    normed = norm(column_order.astype(jnp.int32), tokens, norm_gain, rows, n_p)
    plane = gather_blocks(normed, "sp", p, n_p, plane_of)
    whole = gather_blocks(plane, "tp", tp, n_tp, core_of)
    span = n_p * n_tp * tokens.shape[0]
    whole = whole.transpose(1, 0, 2, 3).reshape(span, width)
    shift = gather_blocks(decay_shift, "sp", p, n_p, plane_of).reshape(span)

    down = w_rank_down.reshape(n_z, n_p, rows, -1)
    down = jnp.stack([lax.dynamic_index_in_dim(down, other, 1, keepdims=False) for other in others], axis=1)
    rank = jnp.dot(whole, down.reshape(width, -1), preferred_element_type=jnp.float32).astype(jnp.bfloat16)
    up = lax.dynamic_slice_in_dim(w_rank_up, p * DK, DK, axis=1)
    bias = lax.dynamic_slice_in_dim(gate_bias, p * DK, DK, axis=0)
    pre = jnp.dot(rank, up, preferred_element_type=jnp.float32) + bias
    cumul, before, to_end, decay = decays(pre, shift)

    owners = jnp.stack([(z - offset) % n_z if offset else z for offset in offsets]).astype(jnp.int32)
    if not short:
        owners = jnp.zeros_like(owners)
    total, early = None, max(len(weights) - 2, 0)
    if early:
        total = project(owners[:early], whole, weights[:early], None)
    if len(weights) > 1:
        total = project(owners[early : early + 1], whole, weights[early : early + 1], total)
    joined, state = close(owners[-1:], whole, weights[-1], total, to_end)
    carried = entering(state, decay[0], n_sp, n_p).astype(jnp.bfloat16)
    near, far = attend(joined, cumul, before)
    order = jnp.stack([partner(tp, step, n_tp) if step else tp for step in range(n_tp)]).astype(jnp.int32)
    shaped = finish(order, near, far, carried, out_gain, n_p, n_tp)

    parts = []
    for columns in cuts:
        sent = []
        for step in range(1, n_tp):
            part = jnp.dot(shaped[step], columns, preferred_element_type=jnp.float32).astype(jnp.bfloat16)
            sent.append(lax.ppermute(part, "tp", core_of(step)))
        mine = jnp.dot(shaped[0], columns, preferred_element_type=jnp.float32)
        for part in sent:
            mine = mine + part.astype(jnp.float32)
        mine = mine.astype(jnp.bfloat16).reshape(n_p, tokens.shape[0], columns.shape[1])
        parts.append(reduce_plane(mine, p, n_sp, n_p, len(parts)))
    if not short:
        return parts[0]
    mixed = jnp.zeros(tokens.shape, jnp.bfloat16)
    block = width // n_z
    pieces = [part[:, i : i + block] for part in parts for i in range(0, part.shape[1], block)]
    for step, part in enumerate(pieces):
        mixed = lax.dynamic_update_slice_in_dim(mixed, part, owners[step] * block, axis=1)
    return mixed


def solution(mesh):
    return jax.shard_map(
        on_device,
        mesh=mesh,
        in_specs=(
            P(("sp", "tp"), None),
            P(),
            P("sp", "tp"),
            P("sp", "tp"),
            P("sp", "tp"),
            P(),
            P(None, "tp"),
            P("tp"),
            P("sp"),
            P(),
            P("tp", "sp"),
        ),
        out_specs=P(("sp", "tp"), None),
        check_vma=False,
    )
```

```python
import functools

import jax
import jax.numpy as jnp
from jax import lax
from jax.experimental import pallas as pl
from jax.experimental.pallas import tpu as pltpu
from jax.sharding import PartitionSpec as P


DK = 256
DV = 512
TAU = 16
BLOCK = 64
EPS = 1e-06
SHORT = 8
RANK_LANES = 128
EXTRA = 16


def partner(index, step, count):
    if count & (count - 1) == 0:
        return index ^ step
    return (step - index) % count


def plane_pairs(n_sp, n_p, step):
    return [(s, s // n_p * n_p + partner(s % n_p, step, n_p)) for s in range(n_sp)]


def line(own, ahead, n_sp, n_p):
    n_z = n_sp // n_p
    up = [(s, (s + n_p) % n_sp) for s in range(n_sp)]
    down = [(s, (s - n_p) % n_sp) for s in range(n_sp)]
    blocks, offsets = [own], [0]
    if n_z > 1:
        if ahead is None:
            ahead = lax.ppermute(own, "sp", up)
        blocks.append(ahead)
        offsets.append(1)
    if n_z > 2:
        blocks.append(lax.ppermute(own, "sp", down))
        offsets.append(n_z - 1)
    for offset in range(2, n_z - 1):
        ahead = lax.ppermute(ahead, "sp", up)
        blocks.append(ahead)
        offsets.append(offset)
    return blocks, offsets


def gather_planes(value, n_sp, n_p):
    lines = [[i + j * n_p for j in range(n_sp // n_p)] for i in range(n_p)]
    return lax.all_gather(value, "sp", axis_index_groups=lines)


def pack_kernel(order_ref, q_ref, k_ref, v_ref, *out_refs):
    for i, out_ref in enumerate(out_refs):
        head = order_ref[i]
        narrow = pl.ds(pl.multiple_of(head * DK, DK), DK)
        wide = pl.ds(pl.multiple_of(head * DV, DV), DV)
        out_ref[:, :DK] = q_ref[:, narrow]
        out_ref[:, DK : 2 * DK] = k_ref[:, narrow]
        out_ref[:, 2 * DK :] = v_ref[:, wide]


def whole_specs(count):
    return [pl.BlockSpec(memory_space=pltpu.VMEM)] * count


def pack(order, w_query, w_key, w_value):
    rows = w_query.shape[0]
    heads = w_query.shape[1] // DK
    return pl.pallas_call(
        pack_kernel,
        in_specs=[pl.BlockSpec(memory_space=pltpu.SMEM)] + whole_specs(3),
        out_specs=whole_specs(heads),
        out_shape=[jax.ShapeDtypeStruct((rows, 2 * DK + DV), jnp.bfloat16)] * heads,
        compiler_params=pltpu.CompilerParams(vmem_limit_bytes=8 << 20),
        name="pack",
    )(order, w_query, w_key, w_value)


def thirds(value):
    high = value.astype(jnp.bfloat16)
    rest = value - high.astype(jnp.float32)
    middle = rest.astype(jnp.bfloat16)
    return high, middle, (rest - middle.astype(jnp.float32)).astype(jnp.bfloat16)


def norm_kernel(order_ref, tokens_ref, gain_ref, down_ref, shift_ref, *refs, rows):
    out_refs, held = refs[:-1], refs[-1]
    wide = tokens_ref[...].astype(jnp.float32)
    scale = lax.rsqrt(jnp.mean(wide * wide, axis=-1, keepdims=True) + EPS)
    held[...] = (wide * scale * gain_ref[...]).astype(jnp.bfloat16)
    width, rank = held.shape[1], down_ref.shape[1]
    tail = mm(held[...], down_ref[...], ((1,), (0,)))
    lane = lax.broadcasted_iota(jnp.int32, tail.shape, 1)
    for i, part in enumerate(thirds(shift_ref[...])):
        tail = jnp.where(lane == rank - 3 + i, part.astype(jnp.float32), tail)
    tail = tail.astype(jnp.bfloat16)
    count = len(out_refs)
    for i, out_ref in enumerate(out_refs):
        out_ref[:, width:] = tail
        if count == 1:
            out_ref[:, :width] = held[...]
            continue
        for block in range(width // rows):
            base, j = block // count * count, block % count
            source = base + order_ref[i * count + j]
            out_ref[:, block * rows : (block + 1) * rows] = held[:, pl.ds(pl.multiple_of(source * rows, rows), rows)]


def norm(order, tokens, gain, down, shift, rows, count):
    shape = (tokens.shape[0], tokens.shape[1] + down.shape[1])
    return pl.pallas_call(
        functools.partial(norm_kernel, rows=rows),
        in_specs=[pl.BlockSpec(memory_space=pltpu.SMEM)] + whole_specs(4),
        out_specs=whole_specs(count),
        out_shape=[jax.ShapeDtypeStruct(shape, jnp.bfloat16)] * count,
        scratch_shapes=[pltpu.VMEM(tokens.shape, jnp.bfloat16)],
        compiler_params=pltpu.CompilerParams(vmem_limit_bytes=12 << 20),
        name="norm",
    )(order, tokens, gain.reshape(1, -1), down, shift.reshape(-1, 1))


def mm(left, right, dims):
    return lax.dot_general(left, right, (dims, ((), ())), preferred_element_type=jnp.float32)


def decays_kernel(order_ref, tail_ref, up_ref, bias_ref, cumul_ref, before_ref, to_end_ref, decay_ref, *, tile):
    rows, rank = tail_ref.shape
    blocks = rows // BLOCK
    row = lax.broadcasted_iota(jnp.int32, (BLOCK, BLOCK), 0)
    column = lax.broadcasted_iota(jnp.int32, (BLOCK, BLOCK), 1)
    lower = jnp.where(row >= column, 1.0, 0.0).astype(jnp.float32)
    pre = mm(tail_ref[...], up_ref[...], ((1,), (0,))) + bias_ref[...]
    shift = jnp.sum(tail_ref[:, rank - 3 :].astype(jnp.float32), axis=1, keepdims=True)
    log_decay = jax.nn.log_sigmoid(pre) / TAU + shift
    for n in range(blocks):
        start = n * BLOCK
        goal = pl.multiple_of(order_ref[start // tile] * tile + start % tile, BLOCK)
        cumul_ref[pl.ds(goal, BLOCK), :] = lax.dot_general(
            lower,
            log_decay[start : start + BLOCK],
            (((1,), (0,)), ((), ())),
            precision=lax.Precision.HIGHEST,
            preferred_element_type=jnp.float32,
        )
    upto = jnp.zeros((1, up_ref.shape[1]), jnp.float32)
    for n in range(blocks):
        before_ref[n : n + 1, :] = upto
        upto = upto + cumul_ref[(n + 1) * BLOCK - 1 : (n + 1) * BLOCK, :]
    decay_ref[...] = jnp.exp(upto)
    for n in range(blocks):
        span = slice(n * BLOCK, (n + 1) * BLOCK)
        to_end_ref[span, :] = jnp.exp((upto - before_ref[n : n + 1, :]) - cumul_ref[span, :])


def decays(order, whole, up, bias):
    rows, (rank, width) = whole.shape[0], up.shape
    last = whole.shape[1] // rank - 1

    def full(*shape):
        return pl.BlockSpec(shape, lambda i, order: (0, 0))

    return pl.pallas_call(
        functools.partial(decays_kernel, tile=rows // order.shape[0]),
        grid_spec=pltpu.PrefetchScalarGridSpec(
            num_scalar_prefetch=1,
            grid=(1,),
            in_specs=[
                pl.BlockSpec((rows, rank), lambda i, order: (0, last)),
                full(rank, width),
                full(1, width),
            ],
            out_specs=[full(rows, width), full(rows // BLOCK, width), full(rows, width), full(1, width)],
        ),
        out_shape=(
            jax.ShapeDtypeStruct((rows, width), jnp.float32),
            jax.ShapeDtypeStruct((rows // BLOCK, width), jnp.float32),
            jax.ShapeDtypeStruct((rows, width), jnp.float32),
            jax.ShapeDtypeStruct((1, width), jnp.float32),
        ),
        compiler_params=pltpu.CompilerParams(vmem_limit_bytes=16 << 20),
        cost_estimate=pl.CostEstimate(flops=1_000_000_000, transcendentals=1_000_000, bytes_accessed=4_000_000),
        name="decays",
    )(order, whole, up, bias.reshape(1, -1))


def project_kernel(index_ref, *refs, count, started):
    parts, blocks, out_ref = refs[:count], refs[count : 2 * count], refs[-1]
    total = sum(mm(x[...], w[...], ((1,), (0,))) for x, w in zip(parts, blocks))
    out_ref[...] = total + refs[2 * count][...] if started else total


def project(index, whole, blocks, total):
    rows, (depth, width), count = whole.shape[0], blocks[0].shape, len(blocks)
    tile = min(rows, 256)

    def part_spec(i):
        return pl.BlockSpec((tile, depth), lambda m, index: (m, index[i]))

    started = total is not None
    return pl.pallas_call(
        functools.partial(project_kernel, count=count, started=started),
        grid_spec=pltpu.PrefetchScalarGridSpec(
            num_scalar_prefetch=1,
            grid=(rows // tile,),
            in_specs=[part_spec(i) for i in range(count)]
            + [pl.BlockSpec((depth, width), lambda m, index: (0, 0))] * count
            + [pl.BlockSpec((tile, width), lambda m, index: (m, 0))] * started,
            out_specs=pl.BlockSpec((tile, width), lambda m, index: (m, 0)),
        ),
        out_shape=jax.ShapeDtypeStruct((rows, width), jnp.float32),
        compiler_params=pltpu.CompilerParams(vmem_limit_bytes=20 << 20),
        cost_estimate=pl.CostEstimate(
            flops=2 * rows * depth * width * count, transcendentals=0, bytes_accessed=8 * rows * width
        ),
        name="project",
    )(index, *([whole] * count), *blocks, *([total] if started else []))


def pack_state(state, decay):
    rows = jnp.concatenate([part.reshape(1, -1) for part in thirds(decay)], axis=0)
    rows = jnp.concatenate([rows, jnp.zeros((EXTRA - 3, rows.shape[1]), rows.dtype)], axis=0)
    return jnp.concatenate([state.astype(jnp.bfloat16), rows], axis=0)


def close_kernel(index_ref, order_ref, part_ref, block_ref, *refs, started, tile):
    to_end_ref, decay_ref, joined_ref, state_ref, packed_ref = refs[-5:]
    total = mm(part_ref[...], block_ref[...], ((1,), (0,)))
    if started:
        total = total + refs[0][...]
    joined = total.astype(jnp.bfloat16)
    step = pl.program_id(0)
    count = part_ref.shape[0] // tile
    added = None
    for i in range(count):
        goal = pl.ds(pl.multiple_of(order_ref[step * count + i] * tile, tile), tile)
        piece = joined[i * tile : (i + 1) * tile]
        joined_ref[goal, :] = piece
        last_k = (piece[:, DK : 2 * DK].astype(jnp.float32) * to_end_ref[goal, :]).astype(jnp.bfloat16)
        more = mm(piece[:, 2 * DK :], last_k, ((0,), (0,)))
        added = more if added is None else added + more

    @pl.when(step == 0)
    def _():
        state_ref[...] = added

    @pl.when(step > 0)
    def _():
        state_ref[...] += added

    @pl.when(step == pl.num_programs(0) - 1)
    def _():
        packed_ref[:DV, :] = state_ref[...].astype(jnp.bfloat16)
        row = lax.broadcasted_iota(jnp.int32, (EXTRA, DK), 0)
        extra = jnp.zeros((EXTRA, DK), jnp.float32)
        for i, part in enumerate(thirds(decay_ref[...])):
            extra = jnp.where(row == i, part.astype(jnp.float32), extra)
        packed_ref[DV:, :] = extra.astype(jnp.bfloat16)


def close(index, order, whole, block, total, to_end, decay):
    rows, (depth, width) = whole.shape[0], block.shape
    tile = rows // order.shape[0]
    started = total is not None
    wide = max(tile, min(rows, 256))

    def full(*shape):
        return pl.BlockSpec(shape, lambda m, index, order: (0, 0))

    return pl.pallas_call(
        functools.partial(close_kernel, started=started, tile=tile),
        grid_spec=pltpu.PrefetchScalarGridSpec(
            num_scalar_prefetch=2,
            grid=(rows // wide,),
            in_specs=[pl.BlockSpec((wide, depth), lambda m, index, order: (m, index[0])), full(depth, width)]
            + [pl.BlockSpec((wide, width), lambda m, index, order: (m, 0))] * started
            + [full(rows, DK), full(1, DK)],
            out_specs=[full(rows, width), full(DV, DK), full(DV + EXTRA, DK)],
        ),
        out_shape=(
            jax.ShapeDtypeStruct((rows, width), jnp.bfloat16),
            jax.ShapeDtypeStruct((DV, DK), jnp.float32),
            jax.ShapeDtypeStruct((DV + EXTRA, DK), jnp.bfloat16),
        ),
        compiler_params=pltpu.CompilerParams(vmem_limit_bytes=28 << 20),
        cost_estimate=pl.CostEstimate(
            flops=2 * rows * depth * width, transcendentals=0, bytes_accessed=8 * rows * width
        ),
        name="close",
    )(index, order, whole, block, *([total] if started else []), to_end, decay)


def reduce_plane(mine, p, n_sp, n_p, cut):
    bits = [1 << i for i in range(n_p.bit_length() - 1)]
    if n_p != 1 << len(bits):
        here = lax.dynamic_index_in_dim(mine, p, 0, keepdims=False).astype(jnp.float32)
        for step in range(1, n_p):
            part = lax.dynamic_index_in_dim(mine, partner(p, step, n_p), 0, keepdims=False)
            here = here + lax.ppermute(part, "sp", plane_pairs(n_sp, n_p, step)).astype(jnp.float32)
        return here.astype(jnp.bfloat16)
    mine = mine.reshape((2,) * len(bits) + mine.shape[1:])
    left = list(reversed(bits))
    for bit in bits if cut % 2 else left[:]:
        axis = left.index(bit)
        side = p // bit % 2
        keep = lax.dynamic_index_in_dim(mine, side, axis, keepdims=False)
        give = lax.dynamic_index_in_dim(mine, 1 - side, axis, keepdims=False)
        got = lax.ppermute(give, "sp", plane_pairs(n_sp, n_p, bit))
        mine = (keep.astype(jnp.float32) + got.astype(jnp.float32)).astype(jnp.bfloat16)
        left.remove(bit)
    return mine


def attend_kernel(joined_ref, cumul_ref, before_ref, near_ref, far_ref, state_ref):
    blocks = joined_ref.shape[0] // BLOCK
    row = lax.broadcasted_iota(jnp.int32, (BLOCK, BLOCK), 0)
    column = lax.broadcasted_iota(jnp.int32, (BLOCK, BLOCK), 1)
    for n in range(blocks):
        span = slice(n * BLOCK, (n + 1) * BLOCK)
        q = joined_ref[span, :DK].astype(jnp.float32) * DK ** (-0.5)
        k = joined_ref[span, DK : 2 * DK].astype(jnp.float32)
        v = joined_ref[span, 2 * DK :]
        cumul = cumul_ref[span, :]
        centre = cumul - cumul[BLOCK // 2 : BLOCK // 2 + 1, :]
        final = cumul[BLOCK - 1 :, :]
        q_scaled = (q * jnp.exp(centre)).astype(jnp.bfloat16)
        k_scaled = (k * jnp.exp(-centre)).astype(jnp.bfloat16)
        scores = mm(q_scaled, k_scaled, ((1,), (1,)))
        scores = jnp.where(row >= column, scores, 0.0).astype(jnp.bfloat16)
        near = mm(scores, v, ((1,), (0,)))
        reach = q * jnp.exp(cumul)
        if n:
            near = near + mm(reach.astype(jnp.bfloat16), state_ref[...].astype(jnp.bfloat16), ((1,), (1,)))
        near_ref[span, :] = near
        far_ref[span, :] = (reach * jnp.exp(before_ref[n : n + 1, :])).astype(jnp.bfloat16)
        if n < blocks - 1:
            decayed = (k * jnp.exp(final - cumul)).astype(jnp.bfloat16)
            added = mm(v, decayed, ((0,), (0,)))
            state_ref[...] = state_ref[...] * jnp.exp(final) + added if n else added


def attend(joined, cumul, before):
    rows = joined.shape[0]
    return pl.pallas_call(
        attend_kernel,
        out_shape=(
            jax.ShapeDtypeStruct((rows, DV), jnp.float32),
            jax.ShapeDtypeStruct((rows, DK), jnp.bfloat16),
        ),
        scratch_shapes=[pltpu.VMEM((DV, DK), jnp.float32)],
        compiler_params=pltpu.CompilerParams(vmem_limit_bytes=12 << 20),
        cost_estimate=pl.CostEstimate(flops=5_000_000_000, transcendentals=2_000_000, bytes_accessed=6_000_000),
        name="attend",
    )(joined, cumul, before)


def finish_kernel(index_ref, near_ref, far_ref, carried_ref, gain_ref, out_ref):
    parts, rows = near_ref.shape[0], near_ref.shape[2]
    for i in range(parts):
        attended = near_ref[i, 0] + mm(far_ref[i, 0], carried_ref[...], ((1,), (1,)))
        scale = lax.rsqrt(jnp.mean(attended * attended, axis=-1, keepdims=True) + EPS)
        out_ref[0, i * rows : (i + 1) * rows, :] = (attended * scale * gain_ref[...]).astype(jnp.bfloat16)


def finish(order, near, far, carried, gain, n_p, n_tp):
    rows = near.shape[0] // (n_p * n_tp)
    return pl.pallas_call(
        finish_kernel,
        grid_spec=pltpu.PrefetchScalarGridSpec(
            num_scalar_prefetch=1,
            grid=(n_tp,),
            in_specs=[
                pl.BlockSpec((n_p, 1, rows, DV), lambda i, order: (0, order[i], 0, 0)),
                pl.BlockSpec((n_p, 1, rows, DK), lambda i, order: (0, order[i], 0, 0)),
                pl.BlockSpec((DV, DK), lambda i, order: (0, 0)),
                pl.BlockSpec((1, DV), lambda i, order: (0, 0)),
            ],
            out_specs=pl.BlockSpec((1, n_p * rows, DV), lambda i, order: (i, 0, 0)),
        ),
        out_shape=jax.ShapeDtypeStruct((n_tp, n_p * rows, DV), jnp.bfloat16),
        compiler_params=pltpu.CompilerParams(vmem_limit_bytes=12 << 20),
        name="finish",
    )(order, near.reshape(n_p, n_tp, rows, DV), far.reshape(n_p, n_tp, rows, DK), carried, gain.reshape(1, DV))


def entering(packed, state, decay, n_sp, n_p):
    n_z = n_sp // n_p
    step = 1
    if n_z > SHORT:
        while step < n_z:
            pairs = [(s, s + step * n_p) for s in range(n_sp - step * n_p)]
            have = lax.axis_index("sp") >= step * n_p
            state, decay = (
                state + decay * lax.ppermute(state, "sp", pairs),
                decay * jnp.where(have, lax.ppermute(decay, "sp", pairs), 1.0),
            )
            step *= 2
        return lax.ppermute(state, "sp", [(s, s + n_p) for s in range(n_sp - n_p)])
    result, passed = jnp.zeros(state.shape, jnp.float32), jnp.ones(decay.shape, jnp.float32)
    while step < n_z:
        pairs = [(s, s + step * n_p) for s in range(n_sp - step * n_p)]
        got = lax.ppermute(packed, "sp", pairs).astype(jnp.float32)
        far = jnp.sum(got[DV : DV + 3], axis=0, keepdims=True)
        result = result + passed * got[:DV]
        if 2 * step < n_z:
            state = state + decay * got[:DV]
            passed, decay = passed * far, decay * far
            packed = pack_state(state, decay)
        step *= 2
    return result


def on_device(
    tokens,
    norm_gain,
    w_query,
    w_key,
    w_value,
    w_rank_down,
    w_rank_up,
    gate_bias,
    decay_shift,
    out_gain,
    w_out,
):
    n_sp, n_tp = lax.axis_size("sp"), lax.axis_size("tp")
    sp, tp = lax.axis_index("sp"), lax.axis_index("tp")
    n_p = w_query.shape[1] // DK
    n_z = n_sp // n_p
    p, z = sp % n_p, sp // n_p
    width = tokens.shape[1]
    groups = [[i * n_p + j for j in range(n_p)] for i in range(n_z)]

    def plane_of(step):
        return plane_pairs(n_sp, n_p, step) if step else None

    def core_of(step):
        return [(t, partner(t, step, n_tp)) for t in range(n_tp)] if step else None

    def exchange(value):
        if n_p == 1:
            return value
        return lax.all_to_all(value, "sp", 0, 0, axis_index_groups=groups, tiled=True)

    def spread(pieces):
        got = [lax.ppermute(piece, "sp", plane_of(step)) if step else piece for step, piece in enumerate(pieces)]
        return jnp.concatenate(got, axis=0)

    rows = w_query.shape[0]
    others = [partner(p, step, n_p) if step else p for step in range(n_p)]
    heads_order = jnp.stack(others).astype(jnp.int32)
    short = n_z <= SHORT
    out_rows = w_out.shape[0] // n_p
    raw = w_out.reshape(n_p, out_rows, w_out.shape[1])
    if short:
        depth = n_p * rows
        later = None
        if n_z > 1:
            ahead = [(s, (s + n_p) % n_sp) for s in range(n_sp)]
            later = [lax.ppermute(w, "sp", ahead) for w in (w_value, w_key, w_query)]
        own = spread(pack(heads_order, w_query, w_key, w_value))
        if later:
            later = spread(pack(heads_order, *reversed(later)))
            raw, later = lax.optimization_barrier((raw, later))
        weights, offsets = line(own, later, n_sp, n_p)
        own = exchange(raw).transpose(1, 0, 2).reshape(out_rows, width // n_z)
        outs, _ = line(own, None, n_sp, n_p)
        half = (n_z + 1) // 2
        cuts = [jnp.concatenate(outs[:half], axis=1)] + outs[half:]
    else:
        depth, offsets = n_sp * rows, [0]
        packed = spread(pack(heads_order, w_query, w_key, w_value))
        weights = [gather_planes(packed, n_sp, n_p).reshape(depth, 2 * DK + DV)]
        wide = gather_planes(exchange(raw), n_sp, n_p).reshape(n_sp, out_rows, w_out.shape[1])
        cuts = [wide.transpose(1, 0, 2).reshape(out_rows, width)]

    column_order = jnp.stack([partner(other, step, n_p) if step else other for other in others for step in range(n_p)])
    down = jnp.pad(w_rank_down, ((0, 0), (0, RANK_LANES - w_rank_down.shape[1])))
    shift = lax.dynamic_slice_in_dim(decay_shift, tp * tokens.shape[0], tokens.shape[0])
    normed = list(norm(column_order.astype(jnp.int32), tokens, norm_gain, down, shift, rows, n_p))
    for step in range(1, n_p):
        normed[step] = lax.ppermute(normed[step], "sp", plane_of(step))
    plane = jnp.concatenate(normed, axis=0)
    whole = [plane]
    for step in range(1, n_tp):
        whole.append(lax.ppermute(plane, "tp", core_of(step)))
    whole = jnp.concatenate(whole, axis=0)
    cores = [partner(tp, step, n_tp) if step else tp for step in range(n_tp)]
    places = jnp.stack([other * n_tp + core for core in cores for other in others]).astype(jnp.int32)
    up = lax.dynamic_slice_in_dim(w_rank_up, p * DK, DK, axis=1)
    up = jnp.pad(up, ((0, RANK_LANES - up.shape[0]), (0, 0)))
    bias = lax.dynamic_slice_in_dim(gate_bias, p * DK, DK, axis=0)
    cumul, before, to_end, decay = decays(places, whole, up, bias)

    owners = jnp.stack([(z - offset) % n_z if offset else z for offset in offsets]).astype(jnp.int32)
    if not short:
        owners = jnp.zeros_like(owners)
    total, early = None, max(len(weights) - 2, 0)
    if early:
        total = project(owners[:early], whole, weights[:early], None)
    if len(weights) > 1:
        total = project(owners[early : early + 1], whole, weights[early : early + 1], total)
    joined, state, packed = close(owners[-1:], places, whole, weights[-1], total, to_end, decay)
    carried = entering(packed, state, decay, n_sp, n_p).astype(jnp.bfloat16)
    near, far = attend(joined, cumul, before)
    order = jnp.stack(cores).astype(jnp.int32)
    shaped = finish(order, near, far, carried, out_gain, n_p, n_tp)

    parts = []
    for columns in cuts:
        sent = []
        for step in range(1, n_tp):
            part = jnp.dot(shaped[step], columns, preferred_element_type=jnp.float32).astype(jnp.bfloat16)
            sent.append(lax.ppermute(part, "tp", core_of(step)))
        mine = jnp.dot(shaped[0], columns, preferred_element_type=jnp.float32)
        for part in sent:
            mine = mine + part.astype(jnp.float32)
        mine = mine.astype(jnp.bfloat16).reshape(n_p, tokens.shape[0], columns.shape[1])
        parts.append(reduce_plane(mine, p, n_sp, n_p, len(parts)))
    if not short:
        return parts[0]
    mixed = jnp.zeros(tokens.shape, jnp.bfloat16)
    block = width // n_z
    pieces = [part[:, i : i + block] for part in parts for i in range(0, part.shape[1], block)]
    for step, part in enumerate(pieces):
        mixed = lax.dynamic_update_slice_in_dim(mixed, part, owners[step] * block, axis=1)
    return mixed


def solution(mesh):
    return jax.shard_map(
        on_device,
        mesh=mesh,
        in_specs=(
            P(("sp", "tp"), None),
            P(),
            P("sp", "tp"),
            P("sp", "tp"),
            P("sp", "tp"),
            P(),
            P(None, "tp"),
            P("tp"),
            P("sp"),
            P(),
            P("tp", "sp"),
        ),
        out_specs=P(("sp", "tp"), None),
        check_vma=False,
    )
```

```python
import functools

import jax
import jax.numpy as jnp
from jax import lax
from jax.experimental import pallas as pl
from jax.experimental.pallas import tpu as pltpu
from jax.sharding import PartitionSpec as P


DK = 256
DV = 512
TAU = 16
BLOCK = 64
EPS = 1e-06
SHORT = 8
RANK_LANES = 128
EXTRA = 16


def partner(index, step, count):
    if count & (count - 1) == 0:
        return index ^ step
    return (step - index) % count


def plane_pairs(n_sp, n_p, step):
    return [(s, s // n_p * n_p + partner(s % n_p, step, n_p)) for s in range(n_sp)]


def line(own, ahead, n_sp, n_p, around):
    n_z = n_sp // n_p
    up = [(s, (s + n_p) % n_sp) for s in range(n_sp)]
    down = [(s, (s - n_p) % n_sp) for s in range(n_sp)]
    blocks, offsets = [own], [0]
    if n_z > 1:
        if ahead is None:
            ahead = lax.ppermute(own, "sp", up)
        blocks.append(ahead)
        offsets.append(1)
    if n_z > 2 and around:
        blocks.append(lax.ppermute(own, "sp", down))
        offsets.append(n_z - 1)
    for offset in range(2, n_z - around):
        ahead = lax.ppermute(ahead, "sp", up)
        blocks.append(ahead)
        offsets.append(offset)
    return blocks, offsets


def gather_planes(value, n_sp, n_p):
    lines = [[i + j * n_p for j in range(n_sp // n_p)] for i in range(n_p)]
    return lax.all_gather(value, "sp", axis_index_groups=lines)


def pack_kernel(order_ref, q_ref, k_ref, v_ref, *out_refs):
    for i, out_ref in enumerate(out_refs):
        head = order_ref[i]
        narrow = pl.ds(pl.multiple_of(head * DK, DK), DK)
        wide = pl.ds(pl.multiple_of(head * DV, DV), DV)
        out_ref[:, :DK] = q_ref[:, narrow]
        out_ref[:, DK : 2 * DK] = k_ref[:, narrow]
        out_ref[:, 2 * DK :] = v_ref[:, wide]


def lay_kernel(order_ref, *refs):
    parts, out_ref = refs[:-1], refs[-1]
    for i, part_ref in enumerate(parts):
        width = part_ref.shape[1]
        out_ref[:, pl.ds(pl.multiple_of(order_ref[i] * width, width), width)] = part_ref[...]


def lay(order, parts):
    if len(parts) == 1:
        return parts[0]
    rows, width = parts[0].shape
    return pl.pallas_call(
        lay_kernel,
        in_specs=[pl.BlockSpec(memory_space=pltpu.SMEM)] + whole_specs(len(parts)),
        out_specs=whole_specs(1)[0],
        out_shape=jax.ShapeDtypeStruct((rows, width * len(parts)), jnp.bfloat16),
        compiler_params=pltpu.CompilerParams(vmem_limit_bytes=8 << 20),
        name="lay",
    )(order, *parts)


def whole_specs(count):
    return [pl.BlockSpec(memory_space=pltpu.VMEM)] * count


def pack(order, w_query, w_key, w_value):
    rows = w_query.shape[0]
    heads = w_query.shape[1] // DK
    return pl.pallas_call(
        pack_kernel,
        in_specs=[pl.BlockSpec(memory_space=pltpu.SMEM)] + whole_specs(3),
        out_specs=whole_specs(heads),
        out_shape=[jax.ShapeDtypeStruct((rows, 2 * DK + DV), jnp.bfloat16)] * heads,
        compiler_params=pltpu.CompilerParams(vmem_limit_bytes=8 << 20),
        name="pack",
    )(order, w_query, w_key, w_value)


def thirds(value):
    high = value.astype(jnp.bfloat16)
    rest = value - high.astype(jnp.float32)
    middle = rest.astype(jnp.bfloat16)
    return high, middle, (rest - middle.astype(jnp.float32)).astype(jnp.bfloat16)


def norm_kernel(order_ref, tokens_ref, gain_ref, down_ref, shift_ref, *refs, rows):
    out_refs, held = refs[:-1], refs[-1]
    wide = tokens_ref[...].astype(jnp.float32)
    scale = lax.rsqrt(jnp.mean(wide * wide, axis=-1, keepdims=True) + EPS)
    held[...] = (wide * scale * gain_ref[...]).astype(jnp.bfloat16)
    width, rank = held.shape[1], down_ref.shape[1]
    tail = mm(held[...], down_ref[...], ((1,), (0,)))
    lane = lax.broadcasted_iota(jnp.int32, tail.shape, 1)
    for i, part in enumerate(thirds(shift_ref[...])):
        tail = jnp.where(lane == rank - 3 + i, part.astype(jnp.float32), tail)
    tail = tail.astype(jnp.bfloat16)
    count = len(out_refs)
    for i, out_ref in enumerate(out_refs):
        out_ref[:, width:] = tail
        if count == 1:
            out_ref[:, :width] = held[...]
            continue
        for block in range(width // rows):
            base, j = block // count * count, block % count
            source = base + order_ref[i * count + j]
            out_ref[:, block * rows : (block + 1) * rows] = held[:, pl.ds(pl.multiple_of(source * rows, rows), rows)]


def norm(order, tokens, gain, down, shift, rows, count):
    shape = (tokens.shape[0], tokens.shape[1] + down.shape[1])
    return pl.pallas_call(
        functools.partial(norm_kernel, rows=rows),
        in_specs=[pl.BlockSpec(memory_space=pltpu.SMEM)] + whole_specs(4),
        out_specs=whole_specs(count),
        out_shape=[jax.ShapeDtypeStruct(shape, jnp.bfloat16)] * count,
        scratch_shapes=[pltpu.VMEM(tokens.shape, jnp.bfloat16)],
        compiler_params=pltpu.CompilerParams(vmem_limit_bytes=12 << 20),
        name="norm",
    )(order, tokens, gain.reshape(1, -1), down, shift.reshape(-1, 1))


def mm(left, right, dims):
    return lax.dot_general(left, right, (dims, ((), ())), preferred_element_type=jnp.float32)


def decays_kernel(order_ref, *refs, tile):
    tail_refs, (up_ref, bias_ref, cumul_ref, before_ref, to_end_ref, decay_ref) = refs[:-6], refs[-6:]
    blocks = cumul_ref.shape[0] // BLOCK
    row = lax.broadcasted_iota(jnp.int32, (BLOCK, BLOCK), 0)
    column = lax.broadcasted_iota(jnp.int32, (BLOCK, BLOCK), 1)
    lower = jnp.where(row >= column, 1.0, 0.0).astype(jnp.float32)
    tail = jnp.concatenate([ref[...] for ref in tail_refs], axis=0)
    pre = mm(tail, up_ref[...], ((1,), (0,))) + bias_ref[...]
    shift = jnp.sum(tail[:, tail.shape[1] - 3 :].astype(jnp.float32), axis=1, keepdims=True)
    log_decay = jax.nn.log_sigmoid(pre) / TAU + shift
    for n in range(blocks):
        start = n * BLOCK
        goal = pl.multiple_of(order_ref[start // tile] * tile + start % tile, BLOCK)
        cumul_ref[pl.ds(goal, BLOCK), :] = lax.dot_general(
            lower,
            log_decay[start : start + BLOCK],
            (((1,), (0,)), ((), ())),
            precision=lax.Precision.HIGHEST,
            preferred_element_type=jnp.float32,
        )
    upto = jnp.zeros((1, up_ref.shape[1]), jnp.float32)
    for n in range(blocks):
        before_ref[n : n + 1, :] = upto
        upto = upto + cumul_ref[(n + 1) * BLOCK - 1 : (n + 1) * BLOCK, :]
    decay_ref[...] = jnp.exp(upto)
    for n in range(blocks):
        span = slice(n * BLOCK, (n + 1) * BLOCK)
        to_end_ref[span, :] = jnp.exp((upto - before_ref[n : n + 1, :]) - cumul_ref[span, :])


def decays(order, halves, up, bias):
    (rank, width), rows = up.shape, sum(half.shape[0] for half in halves)
    last = halves[0].shape[1] // rank - 1

    def full(*shape):
        return pl.BlockSpec(shape, lambda i, order: (0, 0))

    return pl.pallas_call(
        functools.partial(decays_kernel, tile=rows // order.shape[0]),
        grid_spec=pltpu.PrefetchScalarGridSpec(
            num_scalar_prefetch=1,
            grid=(1,),
            in_specs=[
                *[pl.BlockSpec((half.shape[0], rank), lambda i, order: (0, last)) for half in halves],
                full(rank, width),
                full(1, width),
            ],
            out_specs=[full(rows, width), full(rows // BLOCK, width), full(rows, width), full(1, width)],
        ),
        out_shape=(
            jax.ShapeDtypeStruct((rows, width), jnp.float32),
            jax.ShapeDtypeStruct((rows // BLOCK, width), jnp.float32),
            jax.ShapeDtypeStruct((rows, width), jnp.float32),
            jax.ShapeDtypeStruct((1, width), jnp.float32),
        ),
        compiler_params=pltpu.CompilerParams(vmem_limit_bytes=16 << 20),
        cost_estimate=pl.CostEstimate(flops=1_000_000_000, transcendentals=1_000_000, bytes_accessed=4_000_000),
        name="decays",
    )(order, *halves, up, bias.reshape(1, -1))


def project_kernel(index_ref, part_ref, *refs):
    blocks, out_ref = refs[:-1], refs[-1]
    total = None
    for i, block_ref in enumerate(blocks):
        depth = block_ref.shape[0]
        part = part_ref[:, pl.ds(pl.multiple_of(index_ref[i] * depth, depth), depth)]
        more = mm(part, block_ref[...], ((1,), (0,)))
        total = more if total is None else total + more
    out_ref[...] = total


def project(index, part, blocks):
    rows, (depth, width), count = part.shape[0], blocks[0].shape, len(blocks)
    return pl.pallas_call(
        project_kernel,
        in_specs=[pl.BlockSpec(memory_space=pltpu.SMEM)] + whole_specs(1 + count),
        out_specs=whole_specs(1)[0],
        out_shape=jax.ShapeDtypeStruct((rows, width), jnp.float32),
        compiler_params=pltpu.CompilerParams(vmem_limit_bytes=20 << 20),
        cost_estimate=pl.CostEstimate(
            flops=2 * rows * depth * width * count, transcendentals=0, bytes_accessed=8 * rows * width
        ),
        name="project",
    )(index, part, *blocks)


def pack_state(state, decay):
    rows = jnp.concatenate([part.reshape(1, -1) for part in thirds(decay)], axis=0)
    rows = jnp.concatenate([rows, jnp.zeros((EXTRA - 3, rows.shape[1]), rows.dtype)], axis=0)
    return jnp.concatenate([state.astype(jnp.bfloat16), rows], axis=0)


def close_kernel(index_ref, order_ref, *refs, count, started, tile):
    part_refs, total_refs, rest = refs[:count], refs[count : count * (1 + started)], refs[count * (1 + started) :]
    block_ref, to_end_ref, decay_ref, joined_ref, state_ref, packed_ref = rest
    depth, place = block_ref.shape[0], 0
    for half, part_ref in enumerate(part_refs):
        start = index_ref[0] * depth
        total = mm(part_ref[:, pl.ds(pl.multiple_of(start, depth), depth)], block_ref[...], ((1,), (0,)))
        if started:
            total = total + total_refs[half][...]
        joined = total.astype(jnp.bfloat16)
        for i in range(joined.shape[0] // tile):
            goal = pl.ds(pl.multiple_of(order_ref[place] * tile, tile), tile)
            joined_ref[goal, :] = joined[i * tile : (i + 1) * tile]
            place += 1
    last_k = (joined_ref[:, DK : 2 * DK].astype(jnp.float32) * to_end_ref[...]).astype(jnp.bfloat16)
    state = mm(joined_ref[:, 2 * DK :], last_k, ((0,), (0,)))
    state_ref[...] = state
    packed_ref[:DV, :] = state.astype(jnp.bfloat16)
    row = lax.broadcasted_iota(jnp.int32, (EXTRA, DK), 0)
    extra = jnp.zeros((EXTRA, DK), jnp.float32)
    for i, part in enumerate(thirds(decay_ref[...])):
        extra = jnp.where(row == i, part.astype(jnp.float32), extra)
    packed_ref[DV:, :] = extra.astype(jnp.bfloat16)


def close(index, order, halves, totals, block, to_end, decay):
    rows, (depth, width) = to_end.shape[0], block.shape
    return pl.pallas_call(
        functools.partial(close_kernel, count=len(halves), started=bool(totals), tile=rows // order.shape[0]),
        in_specs=[pl.BlockSpec(memory_space=pltpu.SMEM)] * 2 + whole_specs(len(halves) + len(totals) + 3),
        out_specs=whole_specs(3),
        out_shape=(
            jax.ShapeDtypeStruct((rows, width), jnp.bfloat16),
            jax.ShapeDtypeStruct((DV, DK), jnp.float32),
            jax.ShapeDtypeStruct((DV + EXTRA, DK), jnp.bfloat16),
        ),
        compiler_params=pltpu.CompilerParams(vmem_limit_bytes=30 << 20),
        cost_estimate=pl.CostEstimate(
            flops=2 * rows * depth * width, transcendentals=0, bytes_accessed=8 * rows * width
        ),
        name="close",
    )(index, order, *halves, *totals, block, to_end, decay)


def reduce_plane(mine, p, n_sp, n_p, cut, direct):
    bits = [1 << i for i in range(n_p.bit_length() - 1)]
    if direct or n_p != 1 << len(bits):
        here = lax.dynamic_index_in_dim(mine, p, 0, keepdims=False).astype(jnp.float32)
        for step in range(1, n_p):
            part = lax.dynamic_index_in_dim(mine, partner(p, step, n_p), 0, keepdims=False)
            here = here + lax.ppermute(part, "sp", plane_pairs(n_sp, n_p, step)).astype(jnp.float32)
        return here.astype(jnp.bfloat16)
    mine = mine.reshape((2,) * len(bits) + mine.shape[1:])
    left = list(reversed(bits))
    for bit in bits if cut % 2 else left[:]:
        axis = left.index(bit)
        side = p // bit % 2
        keep = lax.dynamic_index_in_dim(mine, side, axis, keepdims=False)
        give = lax.dynamic_index_in_dim(mine, 1 - side, axis, keepdims=False)
        got = lax.ppermute(give, "sp", plane_pairs(n_sp, n_p, bit))
        mine = (keep.astype(jnp.float32) + got.astype(jnp.float32)).astype(jnp.bfloat16)
        left.remove(bit)
    return mine


def attend_kernel(joined_ref, cumul_ref, before_ref, near_ref, far_ref, state_ref):
    blocks = joined_ref.shape[0] // BLOCK
    row = lax.broadcasted_iota(jnp.int32, (BLOCK, BLOCK), 0)
    column = lax.broadcasted_iota(jnp.int32, (BLOCK, BLOCK), 1)
    for n in range(blocks):
        span = slice(n * BLOCK, (n + 1) * BLOCK)
        q = joined_ref[span, :DK].astype(jnp.float32) * DK ** (-0.5)
        k = joined_ref[span, DK : 2 * DK].astype(jnp.float32)
        v = joined_ref[span, 2 * DK :]
        cumul = cumul_ref[span, :]
        centre = cumul - cumul[BLOCK // 2 : BLOCK // 2 + 1, :]
        final = cumul[BLOCK - 1 :, :]
        q_scaled = (q * jnp.exp(centre)).astype(jnp.bfloat16)
        k_scaled = (k * jnp.exp(-centre)).astype(jnp.bfloat16)
        scores = mm(q_scaled, k_scaled, ((1,), (1,)))
        scores = jnp.where(row >= column, scores, 0.0).astype(jnp.bfloat16)
        near = mm(scores, v, ((1,), (0,)))
        reach = q * jnp.exp(cumul)
        if n:
            near = near + mm(reach.astype(jnp.bfloat16), state_ref[...].astype(jnp.bfloat16), ((1,), (1,)))
        near_ref[span, :] = near
        far_ref[span, :] = (reach * jnp.exp(before_ref[n : n + 1, :])).astype(jnp.bfloat16)
        if n < blocks - 1:
            decayed = (k * jnp.exp(final - cumul)).astype(jnp.bfloat16)
            added = mm(v, decayed, ((0,), (0,)))
            state_ref[...] = state_ref[...] * jnp.exp(final) + added if n else added


def attend(joined, cumul, before):
    rows = joined.shape[0]
    return pl.pallas_call(
        attend_kernel,
        out_shape=(
            jax.ShapeDtypeStruct((rows, DV), jnp.float32),
            jax.ShapeDtypeStruct((rows, DK), jnp.bfloat16),
        ),
        scratch_shapes=[pltpu.VMEM((DV, DK), jnp.float32)],
        compiler_params=pltpu.CompilerParams(vmem_limit_bytes=12 << 20),
        cost_estimate=pl.CostEstimate(flops=5_000_000_000, transcendentals=2_000_000, bytes_accessed=6_000_000),
        name="attend",
    )(joined, cumul, before)


def finish_kernel(index_ref, near_ref, far_ref, carried_ref, gain_ref, out_ref):
    parts, rows = near_ref.shape[0], near_ref.shape[2]
    for i in range(parts):
        attended = near_ref[i, 0] + mm(far_ref[i, 0], carried_ref[...], ((1,), (1,)))
        scale = lax.rsqrt(jnp.mean(attended * attended, axis=-1, keepdims=True) + EPS)
        out_ref[0, i * rows : (i + 1) * rows, :] = (attended * scale * gain_ref[...]).astype(jnp.bfloat16)


def finish(order, near, far, carried, gain, n_p, n_tp):
    rows = near.shape[0] // (n_p * n_tp)
    return pl.pallas_call(
        finish_kernel,
        grid_spec=pltpu.PrefetchScalarGridSpec(
            num_scalar_prefetch=1,
            grid=(n_tp,),
            in_specs=[
                pl.BlockSpec((n_p, 1, rows, DV), lambda i, order: (0, order[i], 0, 0)),
                pl.BlockSpec((n_p, 1, rows, DK), lambda i, order: (0, order[i], 0, 0)),
                pl.BlockSpec((DV, DK), lambda i, order: (0, 0)),
                pl.BlockSpec((1, DV), lambda i, order: (0, 0)),
            ],
            out_specs=pl.BlockSpec((1, n_p * rows, DV), lambda i, order: (i, 0, 0)),
        ),
        out_shape=jax.ShapeDtypeStruct((n_tp, n_p * rows, DV), jnp.bfloat16),
        compiler_params=pltpu.CompilerParams(vmem_limit_bytes=12 << 20),
        name="finish",
    )(order, near.reshape(n_p, n_tp, rows, DV), far.reshape(n_p, n_tp, rows, DK), carried, gain.reshape(1, DV))


def entering(packed, state, decay, n_sp, n_p):
    n_z = n_sp // n_p
    step = 1
    if n_z > SHORT:
        while step < n_z:
            pairs = [(s, s + step * n_p) for s in range(n_sp - step * n_p)]
            have = lax.axis_index("sp") >= step * n_p
            state, decay = (
                state + decay * lax.ppermute(state, "sp", pairs),
                decay * jnp.where(have, lax.ppermute(decay, "sp", pairs), 1.0),
            )
            step *= 2
        return lax.ppermute(state, "sp", [(s, s + n_p) for s in range(n_sp - n_p)])
    result, passed = jnp.zeros(state.shape, jnp.float32), jnp.ones(decay.shape, jnp.float32)
    while step < n_z:
        pairs = [(s, s + step * n_p) for s in range(n_sp - step * n_p)]
        got = lax.ppermute(packed, "sp", pairs).astype(jnp.float32)
        far = jnp.sum(got[DV : DV + 3], axis=0, keepdims=True)
        result = result + passed * got[:DV]
        if 2 * step < n_z:
            state = state + decay * got[:DV]
            passed, decay = passed * far, decay * far
            packed = pack_state(state, decay)
        step *= 2
    return result


def on_device(
    tokens,
    norm_gain,
    w_query,
    w_key,
    w_value,
    w_rank_down,
    w_rank_up,
    gate_bias,
    decay_shift,
    out_gain,
    w_out,
):
    n_sp, n_tp = lax.axis_size("sp"), lax.axis_size("tp")
    sp, tp = lax.axis_index("sp"), lax.axis_index("tp")
    n_p = w_query.shape[1] // DK
    n_z = n_sp // n_p
    p, z = sp % n_p, sp // n_p
    width = tokens.shape[1]
    groups = [[i * n_p + j for j in range(n_p)] for i in range(n_z)]

    def plane_of(step):
        return plane_pairs(n_sp, n_p, step) if step else None

    def core_of(step):
        return [(t, partner(t, step, n_tp)) for t in range(n_tp)] if step else None

    def exchange(value):
        if n_p == 1:
            return value
        return lax.all_to_all(value, "sp", 0, 0, axis_index_groups=groups, tiled=True)

    def spread(pieces):
        got = [lax.ppermute(piece, "sp", plane_of(step)) if step else piece for step, piece in enumerate(pieces)]
        return jnp.concatenate(got, axis=0)

    rows = w_query.shape[0]
    others = [partner(p, step, n_p) if step else p for step in range(n_p)]
    heads_order = jnp.stack(others).astype(jnp.int32)
    short = n_z <= SHORT
    out_rows = w_out.shape[0] // n_p
    raw = w_out.reshape(n_p, out_rows, w_out.shape[1])
    if short:
        depth = n_p * rows
        later = None
        if n_z > 1:
            ahead = [(s, (s + n_p) % n_sp) for s in range(n_sp)]
            later = [lax.ppermute(w, "sp", ahead) for w in (w_value, w_key, w_query)]
        own = spread(pack(heads_order, w_query, w_key, w_value))
        if later:
            later = spread(pack(heads_order, *reversed(later)))
        weights, offsets = line(own, later, n_sp, n_p, True)
        parts = []
        for step, other in enumerate(others):
            part = lax.dynamic_index_in_dim(raw, other, 0, keepdims=False)
            parts.append(lax.ppermute(part, "sp", plane_of(step)) if step else part)
        own = lay(heads_order, parts)
        outs, out_offsets = line(own, None, n_sp, n_p, False)
        half = (n_z + 1) // 2
        cuts = [jnp.concatenate(outs[:half], axis=1)] + outs[half:]
    else:
        depth, offsets, out_offsets = n_sp * rows, [0], [0]
        packed = spread(pack(heads_order, w_query, w_key, w_value))
        weights = [gather_planes(packed, n_sp, n_p).reshape(depth, 2 * DK + DV)]
        wide = gather_planes(exchange(raw), n_sp, n_p).reshape(n_sp, out_rows, w_out.shape[1])
        cuts = [wide.transpose(1, 0, 2).reshape(out_rows, width)]

    column_order = jnp.stack([partner(other, step, n_p) if step else other for other in others for step in range(n_p)])
    down = jnp.pad(w_rank_down, ((0, 0), (0, RANK_LANES - w_rank_down.shape[1])))
    shift = lax.dynamic_slice_in_dim(decay_shift, tp * tokens.shape[0], tokens.shape[0])
    normed = list(norm(column_order.astype(jnp.int32), tokens, norm_gain, down, shift, rows, n_p))
    for step in range(1, n_p):
        normed[step] = lax.ppermute(normed[step], "sp", plane_of(step))
    cores = [partner(tp, step, n_tp) if step else tp for step in range(n_tp)]
    split = max(n_p - 1, 1)
    whole, places = [], []
    for low, high in ((0, split), (split, n_p)):
        if low == high:
            continue
        plane = jnp.concatenate(normed[low:high], axis=0)
        for step, core in enumerate(cores):
            whole.append(lax.ppermute(plane, "tp", core_of(step)) if step else plane)
            places += [other * n_tp + core for other in others[low:high]]
    places = jnp.stack(places).astype(jnp.int32)
    up = lax.dynamic_slice_in_dim(w_rank_up, p * DK, DK, axis=1)
    up = jnp.pad(up, ((0, RANK_LANES - up.shape[0]), (0, 0)))
    bias = lax.dynamic_slice_in_dim(gate_bias, p * DK, DK, axis=0)
    cumul, before, to_end, decay = decays(places, whole, up, bias)

    owners = jnp.stack([(z - offset) % n_z if offset else z for offset in offsets]).astype(jnp.int32)
    if not short:
        owners = jnp.zeros_like(owners)
    totals = []
    for part in whole if len(weights) > 1 else []:
        totals.append(project(owners[:-1], part, weights[:-1]))
    joined, state, packed = close(owners[-1:], places, whole, totals, weights[-1], to_end, decay)
    carried = entering(packed, state, decay, n_sp, n_p).astype(jnp.bfloat16)
    near, far = attend(joined, cumul, before)
    order = jnp.stack(cores).astype(jnp.int32)
    shaped = finish(order, near, far, carried, out_gain, n_p, n_tp)

    parts = []
    for cut, columns in enumerate(cuts):
        sent = []
        for step in range(1, n_tp):
            part = jnp.dot(shaped[step], columns, preferred_element_type=jnp.float32).astype(jnp.bfloat16)
            sent.append(lax.ppermute(part, "tp", core_of(step)))
        mine = jnp.dot(shaped[0], columns, preferred_element_type=jnp.float32)
        for part in sent:
            mine = mine + part.astype(jnp.float32)
        mine = mine.astype(jnp.bfloat16).reshape(n_p, tokens.shape[0], columns.shape[1])
        parts.append(reduce_plane(mine, p, n_sp, n_p, cut, cut + 1 == len(cuts)))
    if not short:
        return parts[0]
    mixed = jnp.zeros(tokens.shape, jnp.bfloat16)
    block = width // n_z
    pieces = [part[:, i : i + block] for part in parts for i in range(0, part.shape[1], block)]
    for step, part in enumerate(pieces):
        mixed = lax.dynamic_update_slice_in_dim(mixed, part, (z - out_offsets[step]) % n_z * block, axis=1)
    return mixed


def solution(mesh):
    return jax.shard_map(
        on_device,
        mesh=mesh,
        in_specs=(
            P(("sp", "tp"), None),
            P(),
            P("sp", "tp"),
            P("sp", "tp"),
            P("sp", "tp"),
            P(),
            P(None, "tp"),
            P("tp"),
            P("sp"),
            P(),
            P("tp", "sp"),
        ),
        out_specs=P(("sp", "tp"), None),
        check_vma=False,
    )
```

```python
import functools

import jax
import jax.numpy as jnp
from jax import lax
from jax.experimental import pallas as pl
from jax.experimental.pallas import tpu as pltpu
from jax.sharding import PartitionSpec as P


DK = 256
DV = 512
TAU = 16
BLOCK = 64
EPS = 1e-06
SHORT = 8
RANK_LANES = 128
EXTRA = 16


def partner(index, step, count):
    if count & (count - 1) == 0:
        return index ^ step
    return (step - index) % count


def plane_pairs(n_sp, n_p, step):
    return [(s, s // n_p * n_p + partner(s % n_p, step, n_p)) for s in range(n_sp)]


def line(own, ahead, n_sp, n_p):
    n_z = n_sp // n_p
    up = [(s, (s + n_p) % n_sp) for s in range(n_sp)]
    down = [(s, (s - n_p) % n_sp) for s in range(n_sp)]
    blocks, offsets = [own], [0]
    if n_z > 1:
        blocks.append(ahead)
        offsets.append(1)
    if n_z > 2:
        blocks.append(lax.ppermute(own, "sp", down))
        offsets.append(n_z - 1)
    for offset in range(2, n_z - 1):
        ahead = lax.ppermute(ahead, "sp", up)
        blocks.append(ahead)
        offsets.append(offset)
    return blocks, offsets


def gather_planes(value, n_sp, n_p):
    lines = [[i + j * n_p for j in range(n_sp // n_p)] for i in range(n_p)]
    return lax.all_gather(value, "sp", axis_index_groups=lines)


def pack_kernel(order_ref, q_ref, k_ref, v_ref, *out_refs):
    for i, out_ref in enumerate(out_refs):
        head = order_ref[i]
        narrow = pl.ds(pl.multiple_of(head * DK, DK), DK)
        wide = pl.ds(pl.multiple_of(head * DV, DV), DV)
        out_ref[:, :DK] = q_ref[:, narrow]
        out_ref[:, DK : 2 * DK] = k_ref[:, narrow]
        out_ref[:, 2 * DK :] = v_ref[:, wide]


def lay_kernel(order_ref, *refs):
    parts, out_ref = refs[:-1], refs[-1]
    for i, part_ref in enumerate(parts):
        width = part_ref.shape[1]
        out_ref[:, pl.ds(pl.multiple_of(order_ref[i] * width, width), width)] = part_ref[...]


def lay(order, parts):
    if len(parts) == 1:
        return parts[0]
    rows, width = parts[0].shape
    return pl.pallas_call(
        lay_kernel,
        in_specs=[pl.BlockSpec(memory_space=pltpu.SMEM)] + whole_specs(len(parts)),
        out_specs=whole_specs(1)[0],
        out_shape=jax.ShapeDtypeStruct((rows, width * len(parts)), jnp.bfloat16),
        compiler_params=pltpu.CompilerParams(vmem_limit_bytes=8 << 20),
        name="lay",
    )(order, *parts)


def whole_specs(count):
    return [pl.BlockSpec(memory_space=pltpu.VMEM)] * count


def pack(order, w_query, w_key, w_value):
    rows = w_query.shape[0]
    heads = w_query.shape[1] // DK
    return pl.pallas_call(
        pack_kernel,
        in_specs=[pl.BlockSpec(memory_space=pltpu.SMEM)] + whole_specs(3),
        out_specs=whole_specs(heads),
        out_shape=[jax.ShapeDtypeStruct((rows, 2 * DK + DV), jnp.bfloat16)] * heads,
        compiler_params=pltpu.CompilerParams(vmem_limit_bytes=8 << 20),
        name="pack",
    )(order, w_query, w_key, w_value)


def thirds(value):
    high = value.astype(jnp.bfloat16)
    rest = value - high.astype(jnp.float32)
    middle = rest.astype(jnp.bfloat16)
    return high, middle, (rest - middle.astype(jnp.float32)).astype(jnp.bfloat16)


def norm_kernel(order_ref, tokens_ref, gain_ref, down_ref, shift_ref, *refs, rows):
    out_refs, held = refs[:-1], refs[-1]
    wide = tokens_ref[...].astype(jnp.float32)
    scale = lax.rsqrt(jnp.mean(wide * wide, axis=-1, keepdims=True) + EPS)
    held[...] = (wide * scale * gain_ref[...]).astype(jnp.bfloat16)
    width, rank = held.shape[1], down_ref.shape[1]
    tail = mm(held[...], down_ref[...], ((1,), (0,)))
    lane = lax.broadcasted_iota(jnp.int32, tail.shape, 1)
    for i, part in enumerate(thirds(shift_ref[...])):
        tail = jnp.where(lane == rank - 3 + i, part.astype(jnp.float32), tail)
    tail = tail.astype(jnp.bfloat16)
    count = len(out_refs)
    for i, out_ref in enumerate(out_refs):
        out_ref[:, width:] = tail
        if count == 1:
            out_ref[:, :width] = held[...]
            continue
        for block in range(width // rows):
            base, j = block // count * count, block % count
            source = base + order_ref[i * count + j]
            out_ref[:, block * rows : (block + 1) * rows] = held[:, pl.ds(pl.multiple_of(source * rows, rows), rows)]


def norm(order, tokens, gain, down, shift, rows, count):
    shape = (tokens.shape[0], tokens.shape[1] + down.shape[1])
    return pl.pallas_call(
        functools.partial(norm_kernel, rows=rows),
        in_specs=[pl.BlockSpec(memory_space=pltpu.SMEM)] + whole_specs(4),
        out_specs=whole_specs(count),
        out_shape=[jax.ShapeDtypeStruct(shape, jnp.bfloat16)] * count,
        scratch_shapes=[pltpu.VMEM(tokens.shape, jnp.bfloat16)],
        compiler_params=pltpu.CompilerParams(vmem_limit_bytes=12 << 20),
        name="norm",
    )(order, tokens, gain.reshape(1, -1), down, shift.reshape(-1, 1))


def mm(left, right, dims):
    return lax.dot_general(left, right, (dims, ((), ())), preferred_element_type=jnp.float32)


def decays_kernel(order_ref, *refs, tile):
    tail_refs, (up_ref, bias_ref, cumul_ref, before_ref, to_end_ref, decay_ref) = refs[:-6], refs[-6:]
    blocks = cumul_ref.shape[0] // BLOCK
    row = lax.broadcasted_iota(jnp.int32, (BLOCK, BLOCK), 0)
    column = lax.broadcasted_iota(jnp.int32, (BLOCK, BLOCK), 1)
    lower = jnp.where(row >= column, 1.0, 0.0).astype(jnp.float32)
    tail = jnp.concatenate([ref[...] for ref in tail_refs], axis=0)
    pre = mm(tail, up_ref[...], ((1,), (0,))) + bias_ref[...]
    shift = jnp.sum(tail[:, tail.shape[1] - 3 :].astype(jnp.float32), axis=1, keepdims=True)
    log_decay = jax.nn.log_sigmoid(pre) / TAU + shift
    for n in range(blocks):
        start = n * BLOCK
        goal = pl.multiple_of(order_ref[start // tile] * tile + start % tile, BLOCK)
        cumul_ref[pl.ds(goal, BLOCK), :] = lax.dot_general(
            lower,
            log_decay[start : start + BLOCK],
            (((1,), (0,)), ((), ())),
            precision=lax.Precision.HIGHEST,
            preferred_element_type=jnp.float32,
        )
    upto = jnp.zeros((1, up_ref.shape[1]), jnp.float32)
    for n in range(blocks):
        before_ref[n : n + 1, :] = upto
        upto = upto + cumul_ref[(n + 1) * BLOCK - 1 : (n + 1) * BLOCK, :]
    decay_ref[...] = jnp.exp(upto)
    for n in range(blocks):
        span = slice(n * BLOCK, (n + 1) * BLOCK)
        to_end_ref[span, :] = jnp.exp((upto - before_ref[n : n + 1, :]) - cumul_ref[span, :])


def decays(order, halves, up, bias):
    (rank, width), rows = up.shape, sum(half.shape[0] for half in halves)
    last = halves[0].shape[1] // rank - 1

    def full(*shape):
        return pl.BlockSpec(shape, lambda i, order: (0, 0))

    return pl.pallas_call(
        functools.partial(decays_kernel, tile=rows // order.shape[0]),
        grid_spec=pltpu.PrefetchScalarGridSpec(
            num_scalar_prefetch=1,
            grid=(1,),
            in_specs=[
                *[pl.BlockSpec((half.shape[0], rank), lambda i, order: (0, last)) for half in halves],
                full(rank, width),
                full(1, width),
            ],
            out_specs=[full(rows, width), full(rows // BLOCK, width), full(rows, width), full(1, width)],
        ),
        out_shape=(
            jax.ShapeDtypeStruct((rows, width), jnp.float32),
            jax.ShapeDtypeStruct((rows // BLOCK, width), jnp.float32),
            jax.ShapeDtypeStruct((rows, width), jnp.float32),
            jax.ShapeDtypeStruct((1, width), jnp.float32),
        ),
        compiler_params=pltpu.CompilerParams(vmem_limit_bytes=10 << 20),
        cost_estimate=pl.CostEstimate(flops=1_000_000_000, transcendentals=1_000_000, bytes_accessed=4_000_000),
        name="decays",
    )(order, *halves, up, bias.reshape(1, -1))


def project_kernel(index_ref, *refs, count):
    part_refs, blocks, out_refs = refs[:count], refs[count:-count], refs[-count:]
    total = None
    for i, block_ref in enumerate(blocks):
        depth = block_ref.shape[0]
        span = pl.ds(pl.multiple_of(index_ref[i] * depth, depth), depth)
        part = jnp.concatenate([ref[:, span] for ref in part_refs], axis=0)
        more = mm(part, block_ref[...], ((1,), (0,)))
        total = more if total is None else total + more
    low = 0
    for out_ref in out_refs:
        out_ref[...] = total[low : low + out_ref.shape[0]]
        low += out_ref.shape[0]


def project(index, parts, blocks):
    rows, (depth, width), count = sum(part.shape[0] for part in parts), blocks[0].shape, len(blocks)
    return pl.pallas_call(
        functools.partial(project_kernel, count=len(parts)),
        in_specs=[pl.BlockSpec(memory_space=pltpu.SMEM)] + whole_specs(len(parts) + count),
        out_specs=whole_specs(len(parts)),
        out_shape=[jax.ShapeDtypeStruct((part.shape[0], width), jnp.float32) for part in parts],
        compiler_params=pltpu.CompilerParams(vmem_limit_bytes=12 << 20),
        cost_estimate=pl.CostEstimate(
            flops=2 * rows * depth * width * count, transcendentals=0, bytes_accessed=8 * rows * width
        ),
        name="project",
    )(index, *parts, *blocks)


def pack_state(state, decay):
    rows = jnp.concatenate([part.reshape(1, -1) for part in thirds(decay)], axis=0)
    rows = jnp.concatenate([rows, jnp.zeros((EXTRA - 3, rows.shape[1]), rows.dtype)], axis=0)
    return jnp.concatenate([state.astype(jnp.bfloat16), rows], axis=0)


def close_kernel(index_ref, order_ref, *refs, count, started, tile):
    part_refs, total_refs, rest = refs[:count], refs[count : count * (1 + started)], refs[count * (1 + started) :]
    block_ref, to_end_ref, decay_ref, joined_ref, state_ref, packed_ref = rest
    depth, place = block_ref.shape[0], 0
    for half, part_ref in enumerate(part_refs):
        start = index_ref[0] * depth
        total = mm(part_ref[:, pl.ds(pl.multiple_of(start, depth), depth)], block_ref[...], ((1,), (0,)))
        if started:
            total = total + total_refs[half][...]
        joined = total.astype(jnp.bfloat16)
        for i in range(joined.shape[0] // tile):
            goal = pl.ds(pl.multiple_of(order_ref[place] * tile, tile), tile)
            joined_ref[goal, :] = joined[i * tile : (i + 1) * tile]
            place += 1
    last_k = (joined_ref[:, DK : 2 * DK].astype(jnp.float32) * to_end_ref[...]).astype(jnp.bfloat16)
    state = mm(joined_ref[:, 2 * DK :], last_k, ((0,), (0,)))
    state_ref[...] = state
    packed_ref[:DV, :] = state.astype(jnp.bfloat16)
    row = lax.broadcasted_iota(jnp.int32, (EXTRA, DK), 0)
    extra = jnp.zeros((EXTRA, DK), jnp.float32)
    for i, part in enumerate(thirds(decay_ref[...])):
        extra = jnp.where(row == i, part.astype(jnp.float32), extra)
    packed_ref[DV:, :] = extra.astype(jnp.bfloat16)


def close(index, order, halves, totals, block, to_end, decay):
    rows, (depth, width) = to_end.shape[0], block.shape
    return pl.pallas_call(
        functools.partial(close_kernel, count=len(halves), started=bool(totals), tile=rows // order.shape[0]),
        in_specs=[pl.BlockSpec(memory_space=pltpu.SMEM)] * 2 + whole_specs(len(halves) + len(totals) + 3),
        out_specs=whole_specs(3),
        out_shape=(
            jax.ShapeDtypeStruct((rows, width), jnp.bfloat16),
            jax.ShapeDtypeStruct((DV, DK), jnp.float32),
            jax.ShapeDtypeStruct((DV + EXTRA, DK), jnp.bfloat16),
        ),
        compiler_params=pltpu.CompilerParams(vmem_limit_bytes=18 << 20),
        cost_estimate=pl.CostEstimate(
            flops=2 * rows * depth * width, transcendentals=0, bytes_accessed=8 * rows * width
        ),
        name="close",
    )(index, order, *halves, *totals, block, to_end, decay)


def mix_kernel(order_ref, shaped_ref, *refs, count, arrived, outs):
    pieces, got, out_refs = refs[:count], refs[count : count + arrived], refs[-outs:]
    low = 0
    for piece_ref in pieces:
        span = slice(low, low + piece_ref.shape[1])
        low = span.stop
        total = mm(shaped_ref[0], piece_ref[...], ((1,), (0,)))
        for got_ref in got:
            total = total + got_ref[:, span].astype(jnp.float32)
        if outs == 1:
            out_refs[0][:, span] = total.astype(out_refs[0].dtype)
            continue
        rows = out_refs[0].shape[0]
        for block in range(outs):
            out_refs[block][:, span] = total[block * rows : (block + 1) * rows].astype(out_refs[block].dtype)


def mix(order, shaped, step, pieces, got, outs, kind):
    rows, width = shaped.shape[1], sum(piece.shape[1] for piece in pieces)
    part = rows // outs

    def full(array):
        return pl.BlockSpec(array.shape, lambda i, order: (0, 0))

    return pl.pallas_call(
        functools.partial(mix_kernel, count=len(pieces), arrived=len(got), outs=outs),
        grid_spec=pltpu.PrefetchScalarGridSpec(
            num_scalar_prefetch=1,
            grid=(1,),
            in_specs=[pl.BlockSpec((1, rows, shaped.shape[2]), lambda i, order: (step, 0, 0))]
            + [full(array) for array in (*pieces, *got)],
            out_specs=[pl.BlockSpec((part, width), lambda i, order: (0, 0))] * outs,
        ),
        out_shape=[jax.ShapeDtypeStruct((part, width), kind)] * outs,
        compiler_params=pltpu.CompilerParams(vmem_limit_bytes=10 << 20),
        cost_estimate=pl.CostEstimate(
            flops=2 * rows * width * shaped.shape[2], transcendentals=0, bytes_accessed=4 * rows * width
        ),
        name="mix",
    )(order, shaped, *pieces, *got)


def attend_kernel(joined_ref, cumul_ref, before_ref, near_ref, far_ref, state_ref):
    blocks = joined_ref.shape[0] // BLOCK
    row = lax.broadcasted_iota(jnp.int32, (BLOCK, BLOCK), 0)
    column = lax.broadcasted_iota(jnp.int32, (BLOCK, BLOCK), 1)
    for n in range(blocks):
        span = slice(n * BLOCK, (n + 1) * BLOCK)
        q = joined_ref[span, :DK].astype(jnp.float32) * DK ** (-0.5)
        k = joined_ref[span, DK : 2 * DK].astype(jnp.float32)
        v = joined_ref[span, 2 * DK :]
        cumul = cumul_ref[span, :]
        centre = cumul - cumul[BLOCK // 2 : BLOCK // 2 + 1, :]
        final = cumul[BLOCK - 1 :, :]
        q_scaled = (q * jnp.exp(centre)).astype(jnp.bfloat16)
        k_scaled = (k * jnp.exp(-centre)).astype(jnp.bfloat16)
        scores = mm(q_scaled, k_scaled, ((1,), (1,)))
        scores = jnp.where(row >= column, scores, 0.0).astype(jnp.bfloat16)
        near = mm(scores, v, ((1,), (0,)))
        reach = q * jnp.exp(cumul)
        if n:
            near = near + mm(reach.astype(jnp.bfloat16), state_ref[...].astype(jnp.bfloat16), ((1,), (1,)))
        near_ref[span, :] = near
        far_ref[span, :] = (reach * jnp.exp(before_ref[n : n + 1, :])).astype(jnp.bfloat16)
        if n < blocks - 1:
            decayed = (k * jnp.exp(final - cumul)).astype(jnp.bfloat16)
            added = mm(v, decayed, ((0,), (0,)))
            state_ref[...] = state_ref[...] * jnp.exp(final) + added if n else added


def attend(joined, cumul, before):
    rows = joined.shape[0]
    return pl.pallas_call(
        attend_kernel,
        out_shape=(
            jax.ShapeDtypeStruct((rows, DV), jnp.float32),
            jax.ShapeDtypeStruct((rows, DK), jnp.bfloat16),
        ),
        scratch_shapes=[pltpu.VMEM((DV, DK), jnp.float32)],
        compiler_params=pltpu.CompilerParams(vmem_limit_bytes=12 << 20),
        cost_estimate=pl.CostEstimate(flops=5_000_000_000, transcendentals=2_000_000, bytes_accessed=6_000_000),
        name="attend",
    )(joined, cumul, before)


def finish_kernel(index_ref, near_ref, far_ref, carried_ref, gain_ref, out_ref):
    parts, rows = near_ref.shape[0], near_ref.shape[2]
    cores = pl.num_programs(0)
    for i in range(parts):
        block = index_ref[cores + i]
        attended = near_ref[block, 0] + mm(far_ref[block, 0], carried_ref[...], ((1,), (1,)))
        scale = lax.rsqrt(jnp.mean(attended * attended, axis=-1, keepdims=True) + EPS)
        out_ref[0, i * rows : (i + 1) * rows, :] = (attended * scale * gain_ref[...]).astype(jnp.bfloat16)


def finish(order, near, far, carried, gain, n_p, n_tp):
    rows = near.shape[0] // (n_p * n_tp)
    return pl.pallas_call(
        finish_kernel,
        grid_spec=pltpu.PrefetchScalarGridSpec(
            num_scalar_prefetch=1,
            grid=(n_tp,),
            in_specs=[
                pl.BlockSpec((n_p, 1, rows, DV), lambda i, order: (0, order[i], 0, 0)),
                pl.BlockSpec((n_p, 1, rows, DK), lambda i, order: (0, order[i], 0, 0)),
                pl.BlockSpec((DV, DK), lambda i, order: (0, 0)),
                pl.BlockSpec((1, DV), lambda i, order: (0, 0)),
            ],
            out_specs=pl.BlockSpec((1, n_p * rows, DV), lambda i, order: (i, 0, 0)),
        ),
        out_shape=jax.ShapeDtypeStruct((n_tp, n_p * rows, DV), jnp.bfloat16),
        compiler_params=pltpu.CompilerParams(vmem_limit_bytes=12 << 20),
        name="finish",
    )(order, near.reshape(n_p, n_tp, rows, DV), far.reshape(n_p, n_tp, rows, DK), carried, gain.reshape(1, DV))


def entering(packed, state, decay, n_sp, n_p):
    n_z = n_sp // n_p
    step = 1
    if n_z > SHORT:
        while step < n_z:
            pairs = [(s, s + step * n_p) for s in range(n_sp - step * n_p)]
            have = lax.axis_index("sp") >= step * n_p
            state, decay = (
                state + decay * lax.ppermute(state, "sp", pairs),
                decay * jnp.where(have, lax.ppermute(decay, "sp", pairs), 1.0),
            )
            step *= 2
        return lax.ppermute(state, "sp", [(s, s + n_p) for s in range(n_sp - n_p)])
    result, passed = jnp.zeros(state.shape, jnp.float32), jnp.ones(decay.shape, jnp.float32)
    while step < n_z:
        pairs = [(s, s + step * n_p) for s in range(n_sp - step * n_p)]
        got = lax.ppermute(packed, "sp", pairs).astype(jnp.float32)
        far = jnp.sum(got[DV : DV + 3], axis=0, keepdims=True)
        result = result + passed * got[:DV]
        if 2 * step < n_z:
            state = state + decay * got[:DV]
            passed, decay = passed * far, decay * far
            packed = pack_state(state, decay)
        step *= 2
    return result


def on_device(
    tokens,
    norm_gain,
    w_query,
    w_key,
    w_value,
    w_rank_down,
    w_rank_up,
    gate_bias,
    decay_shift,
    out_gain,
    w_out,
):
    n_sp, n_tp = lax.axis_size("sp"), lax.axis_size("tp")
    sp, tp = lax.axis_index("sp"), lax.axis_index("tp")
    n_p = w_query.shape[1] // DK
    n_z = n_sp // n_p
    p, z = sp % n_p, sp // n_p
    width = tokens.shape[1]
    planes = [[i * n_p + j for j in range(n_p)] for i in range(n_z)]

    def plane_of(step):
        return plane_pairs(n_sp, n_p, step) if step else None

    def core_of(step):
        return [(t, partner(t, step, n_tp)) for t in range(n_tp)] if step else None

    def exchange(value):
        if n_p == 1:
            return value
        return lax.all_to_all(value, "sp", 0, 0, axis_index_groups=planes, tiled=True)

    def spread(pieces):
        got = [lax.ppermute(piece, "sp", plane_of(step)) if step else piece for step, piece in enumerate(pieces)]
        return jnp.concatenate(got, axis=0)

    rows = w_query.shape[0]
    others = [partner(p, step, n_p) if step else p for step in range(n_p)]
    heads_order = jnp.stack(others).astype(jnp.int32)
    short = n_z <= SHORT
    out_rows = w_out.shape[0] // n_p
    raw = w_out.reshape(n_p, out_rows, w_out.shape[1])
    if short:
        depth = n_p * rows
        later = None
        if n_z > 1:
            ahead = [(s, (s + n_p) % n_sp) for s in range(n_sp)]
            later = [lax.ppermute(w, "sp", ahead) for w in (w_value, w_key, w_query)]
        own = spread(pack(heads_order, w_query, w_key, w_value))
        if later:
            later = spread(pack(heads_order, *reversed(later)))
        weights, offsets = line(own, later, n_sp, n_p)
        parts = []
        for step, other in enumerate(others):
            part = lax.dynamic_index_in_dim(raw, other, 0, keepdims=False)
            parts.append(lax.ppermute(part, "sp", plane_of(step)) if step else part)
        own = lay(heads_order, parts)
        block = own.shape[1]
        up = [(s, (s + n_p) % n_sp) for s in range(n_sp)]
        moving, pieces = [own[:, : block // 2], own[:, block // 2 :]], [(0, 0, own)]
        for offset in range(1, n_z):
            for i in range(2):
                moving[i] = lax.ppermute(moving[i], "sp", up)
                pieces.append((offset, i * (block // 2), moving[i]))
        groups = [pieces[:3]] + [pieces[i : i + 2] for i in range(3, len(pieces), 2)]
        cuts = [[piece for _, _, piece in group] for group in groups]
    else:
        depth, offsets = n_sp * rows, [0]
        packed = spread(pack(heads_order, w_query, w_key, w_value))
        weights = [gather_planes(packed, n_sp, n_p).reshape(depth, 2 * DK + DV)]
        wide = gather_planes(exchange(raw), n_sp, n_p).reshape(n_sp, out_rows, w_out.shape[1])
        cuts = [[wide.transpose(1, 0, 2).reshape(out_rows, width)]]

    column_order = jnp.stack([partner(other, step, n_p) if step else other for other in others for step in range(n_p)])
    down = jnp.pad(w_rank_down, ((0, 0), (0, RANK_LANES - w_rank_down.shape[1])))
    shift = lax.dynamic_slice_in_dim(decay_shift, tp * tokens.shape[0], tokens.shape[0])
    normed = list(norm(column_order.astype(jnp.int32), tokens, norm_gain, down, shift, rows, n_p))
    for step in range(1, n_p):
        normed[step] = lax.ppermute(normed[step], "sp", plane_of(step))
    cores = [partner(tp, step, n_tp) if step else tp for step in range(n_tp)]
    split = max(n_p - 1, 1)
    whole, places = [], []
    for low, high in ((0, split), (split, n_p)):
        if low == high:
            continue
        plane = jnp.concatenate(normed[low:high], axis=0)
        for step, core in enumerate(cores):
            whole.append(lax.ppermute(plane, "tp", core_of(step)) if step else plane)
            places += [other * n_tp + core for other in others[low:high]]
    places = jnp.stack(places).astype(jnp.int32)
    up = lax.dynamic_slice_in_dim(w_rank_up, p * DK, DK, axis=1)
    up = jnp.pad(up, ((0, RANK_LANES - up.shape[0]), (0, 0)))
    bias = lax.dynamic_slice_in_dim(gate_bias, p * DK, DK, axis=0)
    cumul, before, to_end, decay = decays(places, whole, up, bias)

    owners = jnp.stack([(z - offset) % n_z if offset else z for offset in offsets]).astype(jnp.int32)
    if not short:
        owners = jnp.zeros_like(owners)
    totals = []
    if len(weights) > 1:
        for part in whole[:n_tp]:
            totals += project(owners[:-1], [part], weights[:-1])
        for part in whole[n_tp:]:
            totals += project(owners[:-1], [part], weights[:-1])
    joined, state, packed = close(owners[-1:], places, whole, totals, weights[-1], to_end, decay)
    carried = entering(packed, state, decay, n_sp, n_p).astype(jnp.bfloat16)
    near, far = attend(joined, cumul, before)
    order = jnp.stack(cores + others).astype(jnp.int32)
    shaped = finish(order, near, far, carried, out_gain, n_p, n_tp)

    parts = []
    for columns in cuts:
        sent = []
        for step in range(1, n_tp):
            part = mix(order, shaped, step, columns, [], 1, jnp.bfloat16)[0]
            sent.append(lax.ppermute(part, "tp", core_of(step)))
        mine = mix(order, shaped, 0, columns, sent, n_p, jnp.bfloat16)
        total = mine[0].astype(jnp.float32)
        for step in range(1, n_p):
            got = lax.ppermute(mine[step], "sp", plane_of(step))
            total = total + got.astype(jnp.float32)
        parts.append(total.astype(jnp.bfloat16))
    if not short:
        return parts[0]
    mixed = jnp.zeros(tokens.shape, jnp.bfloat16)
    for group, part in zip(groups, parts):
        low = 0
        for offset, column, piece in group:
            high = low + piece.shape[1]
            place = (z - offset) % n_z * block + column
            mixed = lax.dynamic_update_slice_in_dim(mixed, part[:, low:high], place, axis=1)
            low = high
    return mixed


def solution(mesh):
    return jax.shard_map(
        on_device,
        mesh=mesh,
        in_specs=(
            P(("sp", "tp"), None),
            P(),
            P("sp", "tp"),
            P("sp", "tp"),
            P("sp", "tp"),
            P(),
            P(None, "tp"),
            P("tp"),
            P("sp"),
            P(),
            P("tp", "sp"),
        ),
        out_specs=P(("sp", "tp"), None),
        check_vma=False,
    )
```
